32 devices in a mesh: fs: 8 (over z, y), tp: 4 (over x, core).
Axes of the slice: x: 2, y: 2, z: 4, core: 2. Of those that a mesh axis runs over, the one named last changes fastest.
Arguments:
- saved_input: bfloat16 [6144, 2048], P('fs'), may hold values from -6 to 6
- cot_inproj: bfloat16 [6144, 1024], P('fs', 'tp'), may hold values from -0.076171875 to 0.076171875
- cot_outproj: bfloat16 [6144, 1024], P('fs', 'tp'), may hold values from -0.076171875 to 0.076171875
- factor_inproj: bfloat16 [2048, 256], P('fs')
- factor_outproj: bfloat16 [2048, 256], P('fs')
- weight_inproj: float32 [2048, 1024], P('fs', 'tp'), may hold values from -0.125 to 0.125
- weight_outproj: float32 [2048, 1024], P('fs', 'tp'), may hold values from -0.125 to 0.125
- first_inproj: float32 [256, 1024], P('fs', 'tp'), may hold values from -6 to 6
- first_outproj: float32 [256, 1024], P('fs', 'tp'), may hold values from -6 to 6
- second_inproj: float32 [256, 1024], P('fs', 'tp'), may hold values from 0.25 to 4
- second_outproj: float32 [256, 1024], P('fs', 'tp'), may hold values from 0.25 to 4
Outputs:
- update_inproj: float32 [2048, 1024], P('fs', 'tp')
- update_outproj: float32 [2048, 1024], P('fs', 'tp')
- new_inproj: float32 [2048, 1024], P('fs', 'tp')
- new_outproj: float32 [2048, 1024], P('fs', 'tp')
- copy_inproj: bfloat16 [2048, 1024], P(None, 'tp')
- copy_outproj: bfloat16 [2048, 1024], P(None, 'tp')
- first_inproj_new: float32 [256, 1024], P('fs', 'tp')
- first_outproj_new: float32 [256, 1024], P('fs', 'tp')
- second_inproj_new: float32 [256, 1024], P('fs', 'tp')
- second_outproj_new: float32 [256, 1024], P('fs', 'tp')
The draws below stay inside these ranges and needn't reach their ends.
All inputs are finite; a program needn't handle non-finite values.
Results may differ from the reference program's by a relative error of at most 0.00045.
Values may be sent and summed in bfloat16 or wider, within the bound.
A program may use at most 64 MiB of HBM per device.

```python
import math
import jax
import jax.numpy as jnp
from jax import lax

D = 2048
RANK = 256
GN = 1024
TOKENS = 6144


def lowrank_draw(key):
    base = jax.random.normal(key, (D, RANK), jnp.float32)
    position = jnp.arange(D).astype(jnp.float32) / D
    scale = jnp.exp(jnp.log(10.0) * position) * 0.22 * D ** (-0.5)
    return (base * scale[:, None]).astype(jnp.bfloat16)


def draw_factor_inproj(key, part):
    return lowrank_draw(jax.random.fold_in(key, 11))


def draw_factor_outproj(key, part):
    return lowrank_draw(jax.random.fold_in(key, 12))


def raised(values, stream_key, source, target, shards_of, factor):
    owner, partner = [(jnp.arange(values.shape[dim]) // (values.shape[dim] // shards_of)).reshape([-1 if axis == dim else 1 for axis in range(values.ndim)]) for dim in (source, target)]
    chosen = jax.random.permutation(stream_key, shards_of)[partner]
    strong = (owner == chosen) | (owner == (partner + shards_of // 2) % shards_of)
    return jnp.where(strong, factor * values, values)


def levels(rng, shape, cuts, least, high):
    level = 1.0
    for axis_at, shards_of in cuts:
        draws = jax.random.uniform(jax.random.fold_in(jax.random.fold_in(rng, 6), axis_at), (shards_of,), jnp.float32, least / len(cuts), high / len(cuts))
        level = level * jnp.repeat(jnp.exp(draws), shape[axis_at] // shards_of).reshape((-1,) + (1,) * (len(shape) - 1 - axis_at))
    return level


def normal_values(key, dims, spread, most, cuts=(), kind=jnp.bfloat16):
    array = spread * jax.random.normal(key, dims, jnp.float32)
    if cuts:
        array = array * levels(key, dims, cuts, -0.22, 0.18)
    return jnp.clip(array, -most, most).astype(kind)


def gaussian_with(stream_key, shape, width, limit, split, heavy, kind=jnp.bfloat16):
    array = width * jax.random.normal(stream_key, shape, jnp.float32)
    if split:
        array = array * levels(stream_key, shape, split, -0.22, 0.18)
    return jnp.clip(raised(array, jax.random.fold_in(stream_key, 3), *heavy), -limit, limit).astype(kind)


def setup_inputs(seed: int = 0) -> dict:
    streams_of = jax.random.split(jax.random.key(seed), 12)
    saved_input = gaussian_with(streams_of[0], (TOKENS, D), 1.0, 6.0, ((0, 8),), (0, 1, 8, 2.0))
    cot_inproj = normal_values(streams_of[1], (TOKENS, GN), (TOKENS ** -0.5), 0.076171875, ((0, 8), (1, 4)))
    cot_outproj = normal_values(streams_of[2], (TOKENS, GN), (TOKENS ** -0.5), 0.076171875, ((0, 8), (1, 4)))
    factor_inproj = draw_factor_inproj(jax.random.fold_in(streams_of[11], 71), 0)
    factor_outproj = draw_factor_outproj(jax.random.fold_in(streams_of[11], 71), 0)
    weight_inproj = normal_values(streams_of[5], (D, GN), D ** -0.5, 0.125, ((0, 8), (1, 4)), jnp.float32)
    weight_outproj = normal_values(streams_of[6], (D, GN), D ** -0.5, 0.125, ((0, 8), (1, 4)), jnp.float32)
    first_inproj = normal_values(streams_of[7], (RANK, GN), 1.0, 6.0, ((0, 8), (1, 4)), jnp.float32)
    first_outproj = normal_values(streams_of[8], (RANK, GN), 1.0, 6.0, ((0, 8), (1, 4)), jnp.float32)
    second_inproj = jnp.clip(jnp.exp(math.log(4.0) - 2.7725887 * jax.random.uniform(streams_of[9], (RANK, GN), jnp.float32) ** levels(streams_of[9], (RANK, GN), ((0, 8), (1, 4)), -0.2, 0.2)), 0.25, 4.0)
    second_outproj = jnp.clip(jnp.exp(math.log(4.0) - 2.7725887 * jax.random.uniform(streams_of[10], (RANK, GN), jnp.float32) ** levels(streams_of[10], (RANK, GN), ((0, 8), (1, 4)), -0.2, 0.2)), 0.25, 4.0)
    return dict(saved_input=saved_input, cot_inproj=cot_inproj, cot_outproj=cot_outproj, factor_inproj=factor_inproj, factor_outproj=factor_outproj, weight_inproj=weight_inproj, weight_outproj=weight_outproj, first_inproj=first_inproj, first_outproj=first_outproj, second_inproj=second_inproj, second_outproj=second_outproj)


def one_matrix(saved_input, cotangent, factor, weight, first, second):
    grad = lax.dot_general(saved_input, cotangent, (((0,), (0,)), ((), ())), preferred_element_type=jnp.float32)
    factor_wide = factor.astype(jnp.float32)
    projected = lax.dot_general(factor_wide, grad, (((0,), (0,)), ((), ())), precision=lax.Precision.HIGHEST)
    first_new = 0.8 * first + 0.2 * projected
    second_new = 0.9 * second + 0.1 * projected * projected
    small = first_new / (jnp.sqrt(second_new) + 1e-08)
    full = jnp.dot(factor_wide, small, precision=lax.Precision.HIGHEST)
    update = full / jnp.sqrt(jnp.mean(full * full) + 1e-06)
    fresh = weight - 0.02 * update
    return (update, fresh, fresh.astype(jnp.bfloat16), first_new, second_new)

def reference(saved_input, cot_inproj, cot_outproj, factor_inproj, factor_outproj, weight_inproj, weight_outproj, first_inproj, first_outproj, second_inproj, second_outproj):
    in_parts = one_matrix(saved_input, cot_inproj, factor_inproj, weight_inproj, first_inproj, second_inproj)
    out_parts = one_matrix(saved_input, cot_outproj, factor_outproj, weight_outproj, first_outproj, second_outproj)
    return (in_parts[0], out_parts[0], in_parts[1], out_parts[1], in_parts[2], out_parts[2], in_parts[3], out_parts[3], in_parts[4], out_parts[4])
```

```python
import functools

import jax
import jax.numpy as jnp
from jax import lax
from jax.experimental import pallas as pl
from jax.experimental.pallas import tpu as pltpu
from jax.sharding import PartitionSpec as P


def contract_rows(left, right, precision):
    return lax.dot_general(
        left,
        right,
        (((0,), (0,)), ((), ())),
        precision=precision,
        preferred_element_type=jnp.float32,
    )


def plain_form(
    saved_input,
    cot_inproj,
    cot_outproj,
    factor_inproj,
    factor_outproj,
    weight_inproj,
    weight_outproj,
    first_inproj,
    first_outproj,
    second_inproj,
    second_outproj,
):
    highest = lax.Precision.HIGHEST
    pieces = (
        lax.all_gather(factor_inproj, "fs", axis=0, tiled=True),
        lax.all_gather(factor_outproj, "fs", axis=0, tiled=True),
    )
    mapped_in = jnp.dot(saved_input, pieces[0], preferred_element_type=jnp.float32)
    mapped_out = jnp.dot(saved_input, pieces[1], preferred_element_type=jnp.float32)
    term_in = contract_rows(mapped_in, cot_inproj.astype(jnp.float32), highest)
    term_out = contract_rows(mapped_out, cot_outproj.astype(jnp.float32), highest)
    projected_in, projected_out = (
        lax.psum_scatter(term_in, "fs", scatter_dimension=0, tiled=True),
        lax.psum_scatter(term_out, "fs", scatter_dimension=0, tiled=True),
    )
    first_in_new = 0.8 * first_inproj + 0.2 * projected_in
    first_out_new = 0.8 * first_outproj + 0.2 * projected_out
    second_in_new = 0.9 * second_inproj + 0.1 * projected_in * projected_in
    second_out_new = 0.9 * second_outproj + 0.1 * projected_out * projected_out
    small_in = first_in_new / (jnp.sqrt(second_in_new) + 1e-08)
    small_out = first_out_new / (jnp.sqrt(second_out_new) + 1e-08)
    wide_in = factor_inproj.astype(jnp.float32)
    wide_out = factor_outproj.astype(jnp.float32)
    pieces = (
        lax.all_gather(small_in, "fs", axis=0, tiled=True),
        lax.all_gather(small_out, "fs", axis=0, tiled=True),
    )
    full_in = jnp.dot(wide_in, pieces[0], precision=highest)
    full_out = jnp.dot(wide_out, pieces[1], precision=highest)
    square_in, square_out = lax.psum(
        (jnp.sum(full_in * full_in), jnp.sum(full_out * full_out)), ("fs", "tp")
    )
    entries = float(full_in.shape[0] * full_in.shape[1] * lax.axis_size("fs") * lax.axis_size("tp"))
    update_in = full_in / jnp.sqrt(square_in / entries + 1e-06)
    update_out = full_out / jnp.sqrt(square_out / entries + 1e-06)
    fresh_in = weight_inproj - 0.02 * update_in
    fresh_out = weight_outproj - 0.02 * update_out
    copy_in, copy_out = (
        lax.all_gather(fresh_in.astype(jnp.bfloat16), "fs", axis=0, tiled=True),
        lax.all_gather(fresh_out.astype(jnp.bfloat16), "fs", axis=0, tiled=True),
    )
    return (
        update_in,
        update_out,
        fresh_in,
        fresh_out,
        copy_in,
        copy_out,
        first_in_new,
        first_out_new,
        second_in_new,
        second_out_new,
    )


MESH = pl.DeviceIdType.MESH
F32, BF16 = jnp.float32, jnp.bfloat16


def parts_of(x):
    high = x.astype(BF16)
    rest = x - high.astype(F32)
    middle = rest.astype(BF16)
    return high, middle, (rest - middle.astype(F32)).astype(BF16)


def dot(a, b):
    return jnp.dot(a, b, preferred_element_type=F32)


class Gather:
    def __init__(self, place, chunks, ref_of, sems):
        self.z, self.y, self.tp, self.depth = place
        self.chunks, self.ref_of = chunks, ref_of
        self.up_s, self.up_r, self.dn_s, self.dn_r, self.y_s, self.y_r = sems

    def copy(self, zi, yi, c, s_sem, r_sem, to_z, to_y):
        ref = self.ref_of(zi * 2 + yi, c)
        return pltpu.make_async_remote_copy(
            src_ref=ref, dst_ref=ref, send_sem=s_sem, recv_sem=r_sem,
            device_id=(to_z * 2 + to_y, self.tp), device_id_type=MESH,
        )

    def up(self, s, c):
        return self.copy(self.z - s, self.y, c, self.up_s.at[s, c], self.up_r.at[s, c], self.z + 1, self.y)

    def down(self, s, c):
        return self.copy(self.z + s, self.y, c, self.dn_s.at[s, c], self.dn_r.at[s, c], self.z - 1, self.y)

    def from_below(self, s, c):
        return self.copy(self.z - 1 - s, self.y, c, self.up_s.at[s, c], self.up_r.at[s, c], self.z, self.y)

    def from_above(self, s, c):
        return self.copy(self.z + 1 + s, self.y, c, self.dn_s.at[s, c], self.dn_r.at[s, c], self.z, self.y)

    def across(self, zi, c):
        return self.copy(zi, self.y, c, self.y_s.at[zi, c], self.y_r.at[zi, c], self.z, 1 - self.y)

    def from_across(self, zi, c):
        return self.copy(zi, 1 - self.y, c, self.y_s.at[zi, c], self.y_r.at[zi, c], self.z, self.y)

    def start(self, c):
        @pl.when(self.z + 1 < self.depth)
        def _():
            self.up(0, c).start()

        @pl.when(self.z >= 1)
        def _():
            self.down(0, c).start()

        self.across(self.z, c).start()

    def relay(self, have=None):
        have = have or (lambda block, c: None)
        for s in range(1, self.depth + 1):
            for c in range(self.chunks):
                if s < self.depth:
                    @pl.when(self.z - s >= 0)
                    def _():
                        self.from_below(s - 1, c).wait_recv()
                        if s < self.depth - 1:
                            @pl.when(self.z + 1 < self.depth)
                            def _():
                                self.up(s, c).start()
                        self.across(self.z - s, c).start()
                        have((self.z - s) * 2 + self.y, c)

                    @pl.when(self.z + s < self.depth)
                    def _():
                        self.from_above(s - 1, c).wait_recv()
                        if s < self.depth - 1:
                            @pl.when(self.z >= 1)
                            def _():
                                self.down(s, c).start()
                        self.across(self.z + s, c).start()
                        have((self.z + s) * 2 + self.y, c)

                if s == 1:
                    self.from_across(self.z, c).wait_recv()
                    have(self.z * 2 + 1 - self.y, c)
                else:
                    @pl.when(self.z - (s - 1) >= 0)
                    def _():
                        self.from_across(self.z - (s - 1), c).wait_recv()
                        have((self.z - (s - 1)) * 2 + 1 - self.y, c)

                    @pl.when(self.z + (s - 1) < self.depth)
                    def _():
                        self.from_across(self.z + (s - 1), c).wait_recv()
                        have((self.z + (s - 1)) * 2 + 1 - self.y, c)

    def finish(self):
        for c in range(self.chunks):
            for s in range(self.depth - 1):
                @pl.when((self.z - s >= 0) & (self.z + 1 < self.depth))
                def _():
                    self.up(s, c).wait_send()

                @pl.when((self.z + s < self.depth) & (self.z >= 1))
                def _():
                    self.down(s, c).wait_send()
            for zi in range(self.depth):
                self.across(zi, c).wait_send()


def gather_sems(depth, chunks):
    dma = pltpu.SemaphoreType.DMA
    return [dma((depth - 1, chunks))] * 4 + [dma((depth, chunks))] * 2


def kernel(
    n, tps, entries,
    saved_hbm, cot_in_hbm, cot_out_hbm, factor_in_hbm, factor_out_hbm, weight_in_hbm, weight_out_hbm,
    first_in_hbm, first_out_hbm, second_in_hbm, second_out_hbm,
    update, fresh, copies, first_new, second_new,
    saved, cots, factors, weights, first, second, mapped, terms, landed, smalls, squares,
    load_sem, f_upS, f_upR, f_dnS, f_dnR, f_yS, f_yR, pair_s, pair_r, term_s, term_r,
    s_upS, s_upR, s_dnS, s_dnR, s_yS, s_yR, norm_s, norm_r,
    c_upS, c_upR, c_dnS, c_dnR, c_yS, c_yR,
):
    me, tp = lax.axis_index("fs"), lax.axis_index("tp")
    z, y = me // 2, me % 2
    depth = n // 2
    side = tp % 2
    partner = tp + 1 - 2 * side
    rows = factors.shape[2]
    slim = first.shape[1]
    place = (z, y, tp, depth)

    barrier = pltpu.get_barrier_semaphore()
    for k in range(1, n):
        pl.semaphore_signal(barrier, inc=1, device_id=((me + k) % n, tp), device_id_type=MESH)
    for k in range(1, tps):
        pl.semaphore_signal(barrier, inc=1, device_id=(me, (tp + k) % tps), device_id_type=MESH)

    loads = [
        pltpu.make_async_copy(source, target, load_sem.at[i])
        for i, (source, target) in enumerate((
            (factor_in_hbm, factors.at[0, me]), (factor_out_hbm, factors.at[1, me]),
            (saved_hbm, saved), (cot_in_hbm, cots.at[0]), (cot_out_hbm, cots.at[1]),
            (first_in_hbm, first.at[0]), (first_out_hbm, first.at[1]),
            (second_in_hbm, second.at[0]), (second_out_hbm, second.at[1]),
            (weight_in_hbm, weights.at[0]), (weight_out_hbm, weights.at[1]),
        ))
    ]
    for load in loads:
        load.start()
    loads[0].wait()
    loads[1].wait()
    pl.semaphore_wait(barrier, n - 1 + tps - 1)

    def hand(block):
        ref = factors.at[side, block]
        return pltpu.make_async_remote_copy(
            src_ref=ref, dst_ref=ref, send_sem=pair_s.at[block], recv_sem=pair_r.at[block],
            device_id=(me, partner), device_id_type=MESH,
        )

    def handed(block):
        ref = factors.at[1 - side, block]
        return pltpu.make_async_remote_copy(
            src_ref=ref, dst_ref=ref, send_sem=pair_s.at[block], recv_sem=pair_r.at[block],
            device_id=(me, tp), device_id_type=MESH,
        )

    gather = Gather(place, 1, lambda block, c: factors.at[side, block], (f_upS, f_upR, f_dnS, f_dnR, f_yS, f_yR))
    gather.start(0)
    loads[2].wait()

    def map_block(block, first_one):
        piece = saved[:, pl.ds(pl.multiple_of(block * rows, rows), rows)]
        for m in range(2):
            product = dot(piece, factors[m, block])
            mapped[m] = product if first_one else mapped[m] + product

    map_block(me, True)
    gather.relay(lambda block, c: hand(block).start())
    for k in range(1, n):
        block = (me + k) % n
        handed(block).wait_recv()
        map_block(block, False)

    for load in loads[3:]:
        load.wait()
    for m in range(2):
        high, middle, low = parts_of(mapped[m].T)
        term = dot(high, cots[m]) + (dot(middle, cots[m]) + dot(low, cots[m]))
        terms[:, m * slim:(m + 1) * slim, :] = term.reshape(n, slim, term.shape[1])

    def send_term(k):
        return pltpu.make_async_remote_copy(
            src_ref=terms.at[(me + k) % n], dst_ref=landed.at[me], send_sem=term_s.at[k], recv_sem=term_r.at[k],
            device_id=((me + k) % n, tp), device_id_type=MESH,
        )

    def recv_term(k):
        return pltpu.make_async_remote_copy(
            src_ref=terms.at[me], dst_ref=landed.at[(me + n - k) % n], send_sem=term_s.at[k], recv_sem=term_r.at[k],
            device_id=(me, tp), device_id_type=MESH,
        )

    for k in range(1, n):
        send_term(k).start()
    projected = terms[me]
    for k in range(1, n):
        recv_term(k).wait_recv()
        projected = projected + landed[(me + n - k) % n]
    for m in range(2):
        here = projected[m * slim:(m + 1) * slim]
        first_m = 0.8 * first[m] + 0.2 * here
        second_m = 0.9 * second[m] + 0.1 * here * here
        first_new[m] = first_m
        second_new[m] = second_m
        smalls[me, m * slim:(m + 1) * slim, :] = first_m / (jnp.sqrt(second_m) + 1e-08)

    small_gather = Gather(place, 1, lambda block, c: smalls.at[block], (s_upS, s_upR, s_dnS, s_dnR, s_yS, s_yR))
    small_gather.start(0)
    small_gather.relay()

    small_parts = [
        parts_of(smalls[:, m * slim:(m + 1) * slim, :].reshape(n * slim, smalls.shape[2])) for m in range(2)
    ]

    def full_of(m, block):
        high, middle, low = small_parts[m]
        factor = factors[m, block]
        return dot(factor, high) + (dot(factor, middle) + dot(factor, low))

    for m in range(2):
        total = None
        for block in range(n):
            full = full_of(m, block)
            square = jnp.sum((full * full).reshape(rows // 8, 8, full.shape[1]), axis=0)
            total = square if total is None else total + square
        squares[tp, m] = total

    def send_square(k):
        return pltpu.make_async_remote_copy(
            src_ref=squares.at[tp], dst_ref=squares.at[tp], send_sem=norm_s.at[k], recv_sem=norm_r.at[k],
            device_id=(me, (tp + k) % tps), device_id_type=MESH,
        )

    def recv_square(k):
        ref = squares.at[(tp + tps - k) % tps]
        return pltpu.make_async_remote_copy(
            src_ref=ref, dst_ref=ref, send_sem=norm_s.at[k], recv_sem=norm_r.at[k],
            device_id=(me, tp), device_id_type=MESH,
        )

    for k in range(1, tps):
        send_square(k).start()
    for m in range(2):
        update[m] = full_of(m, me)
    for k in range(1, tps):
        recv_square(k).wait_recv()
    copy_gather = Gather(place, 2, lambda block, c: copies.at[c, block], (c_upS, c_upR, c_dnS, c_dnR, c_yS, c_yR))
    for m in range(2):
        mean = jnp.sum(jnp.sum(squares[:, m], axis=0), keepdims=True) / entries
        new_update = update[m] / jnp.sqrt(mean + 1e-06)
        update[m] = new_update
        new_weight = weights[m] - 0.02 * new_update
        fresh[m] = new_weight
        copies[m, me] = new_weight.astype(BF16)
        copy_gather.start(m)
    copy_gather.relay()

    gather.finish()
    small_gather.finish()
    copy_gather.finish()
    for k in range(1, n):
        hand((me + k) % n).wait_send()
        send_term(k).wait_send()
    for k in range(1, tps):
        send_square(k).wait_send()


def write_kernel(update, fresh, copies, first_new, second_new, *refs):
    outs, sem = refs[:-1], refs[-1]
    count = 0
    started = []
    for i, source in enumerate((update, fresh, copies, first_new, second_new)):
        for m in range(2):
            copy = pltpu.make_async_copy(source.at[m], outs[2 * i + m], sem.at[count])
            copy.start()
            started.append(copy)
            count += 1
    for copy in started:
        copy.wait()


def kernel_form(n, tps, saved_input, cot_inproj, cot_outproj, factor_inproj, *others):
    tokens, wide = saved_input.shape
    columns = cot_inproj.shape[1]
    rows, rank = factor_inproj.shape
    slim = rank // n
    depth = n // 2
    entries = float(wide * columns * tps)
    dma = pltpu.SemaphoreType.DMA
    vmem = pl.BlockSpec(memory_space=pltpu.VMEM)
    anywhere = pl.BlockSpec(memory_space=pl.ANY)
    shape = jax.ShapeDtypeStruct
    results = pl.pallas_call(
        functools.partial(kernel, n, tps, entries),
        out_shape=(
            shape((2, rows, columns), F32), shape((2, rows, columns), F32),
            shape((2, n, rows, columns), BF16),
            shape((2, slim, columns), F32), shape((2, slim, columns), F32),
        ),
        in_specs=[anywhere] * 11,
        out_specs=[vmem] * 5,
        scratch_shapes=[
            pltpu.VMEM((tokens, wide), BF16),
            pltpu.VMEM((2, tokens, columns), BF16),
            pltpu.VMEM((2, n, rows, rank), BF16),
            pltpu.VMEM((2, rows, columns), F32),
            pltpu.VMEM((2, slim, columns), F32),
            pltpu.VMEM((2, slim, columns), F32),
            pltpu.VMEM((2, tokens, rank), F32),
            pltpu.VMEM((n, 2 * slim, columns), F32),
            pltpu.VMEM((n, 2 * slim, columns), F32),
            pltpu.VMEM((n, 2 * slim, columns), F32),
            pltpu.VMEM((tps, 2, 8, columns), F32),
            dma((11,)),
            *gather_sems(depth, 1), dma((n,)), dma((n,)), dma((n,)), dma((n,)),
            *gather_sems(depth, 1), dma((tps,)), dma((tps,)),
            *gather_sems(depth, 2),
        ],
        compiler_params=pltpu.CompilerParams(collective_id=0, has_side_effects=True, vmem_limit_bytes=48 * 2**20),
    )(saved_input, cot_inproj, cot_outproj, factor_inproj, *others)
    update, fresh, copies, first_new, second_new = results
    copies = copies.reshape(2, n * rows, columns)
    return pl.pallas_call(
        write_kernel,
        out_shape=(
            *[shape((rows, columns), F32)] * 4, *[shape((n * rows, columns), BF16)] * 2, *[shape((slim, columns), F32)] * 4,
        ),
        in_specs=[vmem] * 5,
        out_specs=[anywhere] * 10,
        scratch_shapes=[dma((10,))],
    )(update, fresh, copies, first_new, second_new)


def on_device(saved_input, cot_inproj, cot_outproj, factor_inproj, *others):
    n, tps = lax.axis_size("fs"), lax.axis_size("tp")
    rows, rank = factor_inproj.shape
    if n % 2 == 0 and n >= 4 and tps % 2 == 0 and rank % (8 * n) == 0 and rows % 128 == 0 and cot_inproj.shape[1] % 128 == 0:
        return kernel_form(n, tps, saved_input, cot_inproj, cot_outproj, factor_inproj, *others)
    return plain_form(saved_input, cot_inproj, cot_outproj, factor_inproj, *others)


def solution(mesh):
    return jax.shard_map(
        on_device,
        mesh=mesh,
        in_specs=(
            P("fs", None),
            P("fs", "tp"),
            P("fs", "tp"),
            P("fs", None),
            P("fs", None),
            P("fs", "tp"),
            P("fs", "tp"),
            P("fs", "tp"),
            P("fs", "tp"),
            P("fs", "tp"),
            P("fs", "tp"),
        ),
        out_specs=(
            P("fs", "tp"),
            P("fs", "tp"),
            P("fs", "tp"),
            P("fs", "tp"),
            P(None, "tp"),
            P(None, "tp"),
            P("fs", "tp"),
            P("fs", "tp"),
            P("fs", "tp"),
            P("fs", "tp"),
        ),
        check_vma=False,
    )
```

```python
import functools

import jax
import jax.numpy as jnp
from jax import lax
from jax.experimental import pallas as pl
from jax.experimental.pallas import tpu as pltpu
from jax.sharding import PartitionSpec as P


def contract_rows(left, right, precision):
    return lax.dot_general(
        left,
        right,
        (((0,), (0,)), ((), ())),
        precision=precision,
        preferred_element_type=jnp.float32,
    )


def plain_form(
    saved_input,
    cot_inproj,
    cot_outproj,
    factor_inproj,
    factor_outproj,
    weight_inproj,
    weight_outproj,
    first_inproj,
    first_outproj,
    second_inproj,
    second_outproj,
):
    highest = lax.Precision.HIGHEST
    pieces = (
        lax.all_gather(factor_inproj, "fs", axis=0, tiled=True),
        lax.all_gather(factor_outproj, "fs", axis=0, tiled=True),
    )
    mapped_in = jnp.dot(saved_input, pieces[0], preferred_element_type=jnp.float32)
    mapped_out = jnp.dot(saved_input, pieces[1], preferred_element_type=jnp.float32)
    term_in = contract_rows(mapped_in, cot_inproj.astype(jnp.float32), highest)
    term_out = contract_rows(mapped_out, cot_outproj.astype(jnp.float32), highest)
    projected_in, projected_out = (
        lax.psum_scatter(term_in, "fs", scatter_dimension=0, tiled=True),
        lax.psum_scatter(term_out, "fs", scatter_dimension=0, tiled=True),
    )
    first_in_new = 0.8 * first_inproj + 0.2 * projected_in
    first_out_new = 0.8 * first_outproj + 0.2 * projected_out
    second_in_new = 0.9 * second_inproj + 0.1 * projected_in * projected_in
    second_out_new = 0.9 * second_outproj + 0.1 * projected_out * projected_out
    small_in = first_in_new / (jnp.sqrt(second_in_new) + 1e-08)
    small_out = first_out_new / (jnp.sqrt(second_out_new) + 1e-08)
    wide_in = factor_inproj.astype(jnp.float32)
    wide_out = factor_outproj.astype(jnp.float32)
    pieces = (
        lax.all_gather(small_in, "fs", axis=0, tiled=True),
        lax.all_gather(small_out, "fs", axis=0, tiled=True),
    )
    full_in = jnp.dot(wide_in, pieces[0], precision=highest)
    full_out = jnp.dot(wide_out, pieces[1], precision=highest)
    square_in, square_out = lax.psum(
        (jnp.sum(full_in * full_in), jnp.sum(full_out * full_out)), ("fs", "tp")
    )
    entries = float(full_in.shape[0] * full_in.shape[1] * lax.axis_size("fs") * lax.axis_size("tp"))
    update_in = full_in / jnp.sqrt(square_in / entries + 1e-06)
    update_out = full_out / jnp.sqrt(square_out / entries + 1e-06)
    fresh_in = weight_inproj - 0.02 * update_in
    fresh_out = weight_outproj - 0.02 * update_out
    copy_in, copy_out = (
        lax.all_gather(fresh_in.astype(jnp.bfloat16), "fs", axis=0, tiled=True),
        lax.all_gather(fresh_out.astype(jnp.bfloat16), "fs", axis=0, tiled=True),
    )
    return (
        update_in,
        update_out,
        fresh_in,
        fresh_out,
        copy_in,
        copy_out,
        first_in_new,
        first_out_new,
        second_in_new,
        second_out_new,
    )


MESH = pl.DeviceIdType.MESH
F32, BF16 = jnp.float32, jnp.bfloat16


def parts_of(x):
    high = x.astype(BF16)
    rest = x - high.astype(F32)
    middle = rest.astype(BF16)
    return high, middle, (rest - middle.astype(F32)).astype(BF16)


def dot(a, b):
    return jnp.dot(a, b, preferred_element_type=F32)


class Gather:
    def __init__(self, place, chunks, ref_of, sems):
        self.z, self.y, self.tp, self.depth = place
        self.chunks, self.ref_of = chunks, ref_of
        self.up_s, self.up_r, self.dn_s, self.dn_r, self.y_s, self.y_r, self.x_s, self.x_r = sems

    def detour(self, zi, c):
        z, last = self.z, self.depth - 1
        if self.depth < 4:
            return z < 0
        end = ((z == 1) & (zi == 0)) | ((z == last - 1) & (zi == last))
        if c == self.chunks - 1:
            end = end | ((z == 0) & (zi == 1)) | ((z == last) & (zi == last - 1))
        return end

    def copy(self, zi, yi, c, s_sem, r_sem, to_z, to_y):
        ref = self.ref_of(zi * 2 + yi, c)
        return pltpu.make_async_remote_copy(
            src_ref=ref, dst_ref=ref, send_sem=s_sem, recv_sem=r_sem,
            device_id=(to_z * 2 + to_y, self.tp), device_id_type=MESH,
        )

    def up(self, s, c):
        return self.copy(self.z - s, self.y, c, self.up_s.at[s, c], self.up_r.at[s, c], self.z + 1, self.y)

    def down(self, s, c):
        return self.copy(self.z + s, self.y, c, self.dn_s.at[s, c], self.dn_r.at[s, c], self.z - 1, self.y)

    def from_below(self, s, c):
        return self.copy(self.z - 1 - s, self.y, c, self.up_s.at[s, c], self.up_r.at[s, c], self.z, self.y)

    def from_above(self, s, c):
        return self.copy(self.z + 1 + s, self.y, c, self.dn_s.at[s, c], self.dn_r.at[s, c], self.z, self.y)

    def across(self, zi, c):
        return self.copy(zi, self.y, c, self.y_s.at[zi, c], self.y_r.at[zi, c], self.z, 1 - self.y)

    def from_across(self, zi, c):
        return self.copy(zi, 1 - self.y, c, self.y_s.at[zi, c], self.y_r.at[zi, c], self.z, self.y)

    def beside(self, c, to_z):
        return self.copy(self.z, 1 - self.y, c, self.x_s.at[c], self.x_r.at[c], to_z, self.y)

    def from_beside(self, zi, c):
        return self.copy(zi, 1 - self.y, c, self.x_s.at[c], self.x_r.at[c], self.z, self.y)

    def beside_cases(self, c):
        if self.depth < 4:
            return ()
        z, last = self.z, self.depth - 1
        cases = [(z == 0, 1), (z == last, last - 1)]
        if c == self.chunks - 1:
            cases += [(z == 1, 0), (z == last - 1, last)]
        return cases

    def start(self, c):
        @pl.when(self.z + 1 < self.depth)
        def _():
            self.up(0, c).start()

        @pl.when(self.z >= 1)
        def _():
            self.down(0, c).start()

        self.across(self.z, c).start()

    def hand_on(self, zi, c):
        @pl.when(jnp.logical_not(self.detour(zi, c)))
        def _():
            self.across(zi, c).start()

    def land(self, zi, c, have):
        gone = self.detour(zi, c)

        @pl.when(gone)
        def _():
            self.from_beside(zi, c).wait_recv()

        @pl.when(jnp.logical_not(gone))
        def _():
            self.from_across(zi, c).wait_recv()

        have(zi * 2 + 1 - self.y, c)

    def relay(self, have=None, after=None):
        have = have or (lambda block, c: None)
        z, depth = self.z, self.depth
        for s in range(1, depth + 1):
            for c in range(self.chunks):
                if s < depth:
                    @pl.when(z - s >= 0)
                    def _():
                        self.from_below(s - 1, c).wait_recv()
                        if s < depth - 1:
                            @pl.when(z + 1 < depth)
                            def _():
                                self.up(s, c).start()
                        self.hand_on(z - s, c)
                        have((z - s) * 2 + self.y, c)

                    @pl.when(z + s < depth)
                    def _():
                        self.from_above(s - 1, c).wait_recv()
                        if s < depth - 1:
                            @pl.when(z >= 1)
                            def _():
                                self.down(s, c).start()
                        self.hand_on(z + s, c)
                        have((z + s) * 2 + self.y, c)

                if s == 1:
                    self.from_across(z, c).wait_recv()
                    for condition, neighbour in self.beside_cases(c):
                        @pl.when(condition)
                        def _():
                            self.beside(c, neighbour).start()
                    have(z * 2 + 1 - self.y, c)
                else:
                    @pl.when(z - (s - 1) >= 0)
                    def _():
                        self.land(z - (s - 1), c, have)

                    @pl.when(z + (s - 1) < depth)
                    def _():
                        self.land(z + (s - 1), c, have)
            if after is not None:
                after(s)

    def finish(self):
        for c in range(self.chunks):
            for s in range(self.depth - 1):
                @pl.when((self.z - s >= 0) & (self.z + 1 < self.depth))
                def _():
                    self.up(s, c).wait_send()

                @pl.when((self.z + s < self.depth) & (self.z >= 1))
                def _():
                    self.down(s, c).wait_send()
            for zi in range(self.depth):
                @pl.when(jnp.logical_not(self.detour(zi, c)))
                def _():
                    self.across(zi, c).wait_send()
            for condition, neighbour in self.beside_cases(c):
                @pl.when(condition)
                def _():
                    self.beside(c, neighbour).wait_send()


def gather_sems(depth, chunks):
    dma = pltpu.SemaphoreType.DMA
    return [dma((depth - 1, chunks))] * 4 + [dma((depth, chunks))] * 2 + [dma((chunks,))] * 2


def kernel(
    n, tps, entries,
    saved_hbm, cot_in_hbm, cot_out_hbm, factor_in_hbm, factor_out_hbm, weight_in_hbm, weight_out_hbm,
    first_in_hbm, first_out_hbm, second_in_hbm, second_out_hbm,
    update, fresh, copies, first_new, second_new,
    saved, cots, factors, weights, first, second, mapped, terms, crossed, staged, landed, smalls, squares,
    load_sem, pair_s, pair_r, ty_s, ty_r, tz_s, tz_r, sz_s, sz_r, sy_s, sy_r, norm_s, norm_r, *gather_refs,
):
    me, tp = lax.axis_index("fs"), lax.axis_index("tp")
    z, y = me // 2, me % 2
    depth = n // 2
    side = tp % 2
    partner = tp + 1 - 2 * side
    rows = factors.shape[2]
    half = rows // 2
    slim = first.shape[1]
    place = (z, y, tp, depth)

    barrier = pltpu.get_barrier_semaphore()
    for k in range(1, depth):
        pl.semaphore_signal(barrier, inc=1, device_id=((z + k) % depth * 2 + y, tp), device_id_type=MESH)
    pl.semaphore_signal(barrier, inc=1, device_id=(z * 2 + 1 - y, tp), device_id_type=MESH)
    for k in range(1, tps):
        pl.semaphore_signal(barrier, inc=1, device_id=(me, (tp + k) % tps), device_id_type=MESH)

    loads = [
        pltpu.make_async_copy(source, target, load_sem.at[i])
        for i, (source, target) in enumerate((
            (factor_in_hbm, factors.at[0, me]), (factor_out_hbm, factors.at[1, me]),
            (saved_hbm, saved), (cot_in_hbm, cots.at[0]), (cot_out_hbm, cots.at[1]),
            (first_in_hbm, first.at[0]), (first_out_hbm, first.at[1]),
            (second_in_hbm, second.at[0]), (second_out_hbm, second.at[1]),
            (weight_in_hbm, weights.at[0]), (weight_out_hbm, weights.at[1]),
        ))
    ]
    for load in loads:
        load.start()
    loads[0].wait()
    loads[1].wait()
    pl.semaphore_wait(barrier, depth + tps - 1)

    def factor_ref(m, block, c):
        return factors.at[m, block, pl.ds(c * half, half)]

    def hand(m, block, c):
        ref = factor_ref(m, block, c)
        return pltpu.make_async_remote_copy(
            src_ref=ref, dst_ref=ref, send_sem=pair_s.at[block, c], recv_sem=pair_r.at[block, c],
            device_id=(me, partner), device_id_type=MESH,
        )

    gather = Gather(place, 2, lambda block, c: factor_ref(side, block, c), gather_refs[:8])
    gather.start(0)
    gather.start(1)
    loads[2].wait()

    def map_block(block, first_one=False):
        piece = saved[:, pl.ds(pl.multiple_of(block * rows, rows), rows)]
        for m in range(2):
            product = dot(piece, factors[m, block])
            mapped[m] = product if first_one else mapped[m] + product

    def map_handed(block):
        for c in range(2):
            hand(1 - side, block, c).wait_recv()
        map_block(block)

    def map_at(distance):
        if distance == 0:
            map_handed(z * 2 + 1 - y)
            return

        @pl.when(z - distance >= 0)
        def _():
            map_handed((z - distance) * 2 + y)
            map_handed((z - distance) * 2 + 1 - y)

        @pl.when(z + distance < depth)
        def _():
            map_handed((z + distance) * 2 + y)
            map_handed((z + distance) * 2 + 1 - y)

    map_block(me, True)
    gather.relay(
        lambda block, c: hand(side, block, c).start(),
        lambda s: map_at(s - 2) if s >= 2 else None,
    )
    map_at(depth - 1)

    def term_cross(m, zi):
        return pltpu.make_async_remote_copy(
            src_ref=terms.at[m, zi * 2 + 1 - y], dst_ref=crossed.at[m, zi],
            send_sem=ty_s.at[m, zi], recv_sem=ty_r.at[m, zi],
            device_id=(z * 2 + 1 - y, tp), device_id_type=MESH,
        )

    def term_along(m, zi):
        return pltpu.make_async_remote_copy(
            src_ref=staged.at[m, zi], dst_ref=landed.at[m, z], send_sem=tz_s.at[m, zi], recv_sem=tz_r.at[m, z],
            device_id=(zi * 2 + y, tp), device_id_type=MESH,
        )

    def term_from(m, zi):
        return pltpu.make_async_remote_copy(
            src_ref=staged.at[m, z], dst_ref=landed.at[m, zi], send_sem=tz_s.at[m, z], recv_sem=tz_r.at[m, zi],
            device_id=(z * 2 + y, tp), device_id_type=MESH,
        )

    order = [k % depth for k in range(1, depth + 1)]
    for load in loads[3:]:
        load.wait()
    for m in range(2):
        high, middle, low = parts_of(mapped[m].T)
        term = dot(high, cots[m]) + (dot(middle, cots[m]) + dot(low, cots[m]))
        terms[m] = term.reshape(n, slim, term.shape[1])
        for k in order:
            term_cross(m, (z + k) % depth).start()
    for m in range(2):
        for k in order:
            zi = (z + k) % depth
            term_cross(m, zi).wait_recv()
            staged[m, zi] = terms[m, zi * 2 + y] + crossed[m, zi]
            if k:
                term_along(m, zi).start()

    def small_along(m, zi):
        ref = smalls.at[m, me]
        return pltpu.make_async_remote_copy(
            src_ref=ref, dst_ref=ref, send_sem=sz_s.at[m, zi], recv_sem=sz_r.at[m, z],
            device_id=(zi * 2 + y, tp), device_id_type=MESH,
        )

    def small_from(m, zi):
        ref = smalls.at[m, zi * 2 + y]
        return pltpu.make_async_remote_copy(
            src_ref=ref, dst_ref=ref, send_sem=sz_s.at[m, zi], recv_sem=sz_r.at[m, zi],
            device_id=(z * 2 + y, tp), device_id_type=MESH,
        )

    def small_cross(m, zi, column):
        ref = smalls.at[m, zi * 2 + column]
        return pltpu.make_async_remote_copy(
            src_ref=ref, dst_ref=ref, send_sem=sy_s.at[m, zi], recv_sem=sy_r.at[m, zi],
            device_id=(z * 2 + 1 - y, tp), device_id_type=MESH,
        )

    for m in range(2):
        here = staged[m, z]
        for k in range(1, depth):
            term_from(m, (z + k) % depth).wait_recv()
            here = here + landed[m, (z + k) % depth]
        first_m = 0.8 * first[m] + 0.2 * here
        second_m = 0.9 * second[m] + 0.1 * here * here
        first_new[m] = first_m
        second_new[m] = second_m
        smalls[m, me] = first_m / (jnp.sqrt(second_m) + 1e-08)
        for k in range(1, depth):
            small_along(m, (z + k) % depth).start()
        small_cross(m, z, y).start()
    for m in range(2):
        for k in range(1, depth):
            zi = (z + k) % depth
            small_from(m, zi).wait_recv()
            small_cross(m, zi, y).start()

    def send_square(m, k):
        return pltpu.make_async_remote_copy(
            src_ref=squares.at[m, tp], dst_ref=squares.at[m, tp], send_sem=norm_s.at[m, k], recv_sem=norm_r.at[m, k],
            device_id=(me, (tp + k) % tps), device_id_type=MESH,
        )

    def recv_square(m, k):
        ref = squares.at[m, (tp + tps - k) % tps]
        return pltpu.make_async_remote_copy(
            src_ref=ref, dst_ref=ref, send_sem=norm_s.at[m, k], recv_sem=norm_r.at[m, k],
            device_id=(me, tp), device_id_type=MESH,
        )

    for m in range(2):
        for k in range(depth):
            small_cross(m, (z + k) % depth, 1 - y).wait_recv()
        high, middle, low = parts_of(smalls[m].reshape(n * slim, smalls.shape[3]))

        def full_of(block):
            factor = factors[m, block]
            return dot(factor, high) + (dot(factor, middle) + dot(factor, low))

        total = None
        for block in range(n):
            full = full_of(block)
            square = jnp.sum((full * full).reshape(rows // 8, 8, full.shape[1]), axis=0)
            total = square if total is None else total + square
        squares[m, tp] = total
        for k in range(1, tps):
            send_square(m, k).start()
        update[m] = full_of(me)

    copy_gather = Gather(place, 2, lambda block, c: copies.at[c, block], gather_refs[8:])
    for m in range(2):
        for k in range(1, tps):
            recv_square(m, k).wait_recv()
        mean = jnp.sum(jnp.sum(squares[m], axis=0), keepdims=True) / entries
        new_update = update[m] / jnp.sqrt(mean + 1e-06)
        update[m] = new_update
        new_weight = weights[m] - 0.02 * new_update
        fresh[m] = new_weight
        copies[m, me] = new_weight.astype(BF16)
        copy_gather.start(m)
    copy_gather.relay()

    gather.finish()
    copy_gather.finish()
    for k in range(1, n):
        for c in range(2):
            hand(side, (me + k) % n, c).wait_send()
    for m in range(2):
        for k in range(depth):
            zi = (z + k) % depth
            term_cross(m, zi).wait_send()
            small_cross(m, zi, y).wait_send()
            if k:
                term_along(m, zi).wait_send()
                small_along(m, zi).wait_send()
        for k in range(1, tps):
            send_square(m, k).wait_send()


def write_kernel(update, fresh, copies, first_new, second_new, *refs):
    outs, sem = refs[:-1], refs[-1]
    started = []
    for i, source in enumerate((update, fresh, copies, first_new, second_new)):
        for m in range(2):
            copy = pltpu.make_async_copy(source.at[m], outs[2 * i + m], sem.at[2 * i + m])
            copy.start()
            started.append(copy)
    for copy in started:
        copy.wait()


def kernel_form(n, tps, saved_input, cot_inproj, cot_outproj, factor_inproj, *others):
    tokens, wide = saved_input.shape
    columns = cot_inproj.shape[1]
    rows, rank = factor_inproj.shape
    slim = rank // n
    depth = n // 2
    entries = float(wide * columns * tps)
    dma = pltpu.SemaphoreType.DMA
    vmem = pl.BlockSpec(memory_space=pltpu.VMEM)
    anywhere = pl.BlockSpec(memory_space=pl.ANY)
    far = pl.BlockSpec(memory_space=pltpu.HBM)
    shape = jax.ShapeDtypeStruct
    results = pl.pallas_call(
        functools.partial(kernel, n, tps, entries),
        out_shape=(
            shape((2, rows, columns), F32), shape((2, rows, columns), F32),
            shape((2, n, rows, columns), BF16),
            shape((2, slim, columns), F32), shape((2, slim, columns), F32),
        ),
        in_specs=[far] * 11,
        out_specs=[vmem] * 5,
        scratch_shapes=[
            pltpu.VMEM((tokens, wide), BF16),
            pltpu.VMEM((2, tokens, columns), BF16),
            pltpu.VMEM((2, n, rows, rank), BF16),
            pltpu.VMEM((2, rows, columns), F32),
            pltpu.VMEM((2, slim, columns), F32),
            pltpu.VMEM((2, slim, columns), F32),
            pltpu.VMEM((2, tokens, rank), F32),
            pltpu.VMEM((2, n, slim, columns), F32),
            pltpu.VMEM((2, depth, slim, columns), F32),
            pltpu.VMEM((2, depth, slim, columns), F32),
            pltpu.VMEM((2, depth, slim, columns), F32),
            pltpu.VMEM((2, n, slim, columns), F32),
            pltpu.VMEM((2, tps, 8, columns), F32),
            dma((11,)),
            dma((n, 2)), dma((n, 2)),
            *[dma((2, depth))] * 8,
            dma((2, tps)), dma((2, tps)),
            *gather_sems(depth, 2), *gather_sems(depth, 2),
        ],
        compiler_params=pltpu.CompilerParams(collective_id=0, has_side_effects=True, vmem_limit_bytes=40 * 2**20),
    )(*[pltpu.with_memory_space_constraint(x, pltpu.HBM) for x in (saved_input, cot_inproj, cot_outproj, factor_inproj, *others)])
    update, fresh, copies, first_new, second_new = results
    copies = copies.reshape(2, n * rows, columns)
    return pl.pallas_call(
        write_kernel,
        out_shape=(
            *[shape((rows, columns), F32)] * 4, *[shape((n * rows, columns), BF16)] * 2, *[shape((slim, columns), F32)] * 4,
        ),
        in_specs=[anywhere] * 5,
        out_specs=[far] * 10,
        scratch_shapes=[dma((10,))],
        compiler_params=pltpu.CompilerParams(vmem_limit_bytes=2**20),
    )(update, fresh, copies, first_new, second_new)


def on_device(saved_input, cot_inproj, cot_outproj, factor_inproj, *others):
    n, tps = lax.axis_size("fs"), lax.axis_size("tp")
    rows, rank = factor_inproj.shape
    if n % 2 == 0 and n >= 4 and tps % 2 == 0 and rank % (8 * n) == 0 and rows % 128 == 0 and cot_inproj.shape[1] % 128 == 0:
        return kernel_form(n, tps, saved_input, cot_inproj, cot_outproj, factor_inproj, *others)
    return plain_form(saved_input, cot_inproj, cot_outproj, factor_inproj, *others)


def solution(mesh):
    return jax.shard_map(
        on_device,
        mesh=mesh,
        in_specs=(
            P("fs", None),
            P("fs", "tp"),
            P("fs", "tp"),
            P("fs", None),
            P("fs", None),
            P("fs", "tp"),
            P("fs", "tp"),
            P("fs", "tp"),
            P("fs", "tp"),
            P("fs", "tp"),
            P("fs", "tp"),
        ),
        out_specs=(
            P("fs", "tp"),
            P("fs", "tp"),
            P("fs", "tp"),
            P("fs", "tp"),
            P(None, "tp"),
            P(None, "tp"),
            P("fs", "tp"),
            P("fs", "tp"),
            P("fs", "tp"),
            P("fs", "tp"),
        ),
        check_vma=False,
    )
```

```python
import functools

import jax
import jax.numpy as jnp
from jax import lax
from jax.experimental import pallas as pl
from jax.experimental.pallas import tpu as pltpu
from jax.sharding import PartitionSpec as P


def contract_rows(left, right, precision):
    return lax.dot_general(
        left,
        right,
        (((0,), (0,)), ((), ())),
        precision=precision,
        preferred_element_type=jnp.float32,
    )


def plain_form(
    saved_input,
    cot_inproj,
    cot_outproj,
    factor_inproj,
    factor_outproj,
    weight_inproj,
    weight_outproj,
    first_inproj,
    first_outproj,
    second_inproj,
    second_outproj,
):
    highest = lax.Precision.HIGHEST
    pieces = (
        lax.all_gather(factor_inproj, "fs", axis=0, tiled=True),
        lax.all_gather(factor_outproj, "fs", axis=0, tiled=True),
    )
    mapped_in = jnp.dot(saved_input, pieces[0], preferred_element_type=jnp.float32)
    mapped_out = jnp.dot(saved_input, pieces[1], preferred_element_type=jnp.float32)
    term_in = contract_rows(mapped_in, cot_inproj.astype(jnp.float32), highest)
    term_out = contract_rows(mapped_out, cot_outproj.astype(jnp.float32), highest)
    projected_in, projected_out = (
        lax.psum_scatter(term_in, "fs", scatter_dimension=0, tiled=True),
        lax.psum_scatter(term_out, "fs", scatter_dimension=0, tiled=True),
    )
    first_in_new = 0.8 * first_inproj + 0.2 * projected_in
    first_out_new = 0.8 * first_outproj + 0.2 * projected_out
    second_in_new = 0.9 * second_inproj + 0.1 * projected_in * projected_in
    second_out_new = 0.9 * second_outproj + 0.1 * projected_out * projected_out
    small_in = first_in_new / (jnp.sqrt(second_in_new) + 1e-08)
    small_out = first_out_new / (jnp.sqrt(second_out_new) + 1e-08)
    wide_in = factor_inproj.astype(jnp.float32)
    wide_out = factor_outproj.astype(jnp.float32)
    pieces = (
        lax.all_gather(small_in, "fs", axis=0, tiled=True),
        lax.all_gather(small_out, "fs", axis=0, tiled=True),
    )
    full_in = jnp.dot(wide_in, pieces[0], precision=highest)
    full_out = jnp.dot(wide_out, pieces[1], precision=highest)
    square_in, square_out = lax.psum(
        (jnp.sum(full_in * full_in), jnp.sum(full_out * full_out)), ("fs", "tp")
    )
    entries = float(full_in.shape[0] * full_in.shape[1] * lax.axis_size("fs") * lax.axis_size("tp"))
    update_in = full_in / jnp.sqrt(square_in / entries + 1e-06)
    update_out = full_out / jnp.sqrt(square_out / entries + 1e-06)
    fresh_in = weight_inproj - 0.02 * update_in
    fresh_out = weight_outproj - 0.02 * update_out
    copy_in, copy_out = (
        lax.all_gather(fresh_in.astype(jnp.bfloat16), "fs", axis=0, tiled=True),
        lax.all_gather(fresh_out.astype(jnp.bfloat16), "fs", axis=0, tiled=True),
    )
    return (
        update_in,
        update_out,
        fresh_in,
        fresh_out,
        copy_in,
        copy_out,
        first_in_new,
        first_out_new,
        second_in_new,
        second_out_new,
    )


MESH = pl.DeviceIdType.MESH
F32, BF16 = jnp.float32, jnp.bfloat16


def parts_of(x):
    high = x.astype(BF16)
    rest = x - high.astype(F32)
    middle = rest.astype(BF16)
    return high, middle, (rest - middle.astype(F32)).astype(BF16)


def dot(a, b):
    return jnp.dot(a, b, preferred_element_type=F32)


class Gather:
    def goes_up(self, s):
        z, last = self.z, self.depth - 1
        needed = (z - s >= 0) & (z < last)
        return needed & (z != last - 1) if self.near and s == 0 else needed

    def goes_down(self, s):
        z, last = self.z, self.depth - 1
        needed = (z + s <= last) & (z >= 1)
        return needed & (z != 1) if self.near and s == 0 else needed

    def crosses(self, zi, c):
        sent = jnp.logical_not(self.detour(zi, c))
        return sent & (zi != self.z) if self.near else sent

    def __init__(self, place, chunks, ref_of, sems, near=False):
        self.z, self.y, self.tp, self.depth = place
        self.near = near
        self.chunks, self.ref_of = chunks, ref_of
        self.up_s, self.up_r, self.dn_s, self.dn_r, self.y_s, self.y_r, self.x_s, self.x_r = sems

    def detour(self, zi, c):
        z, last = self.z, self.depth - 1
        if self.depth < 4:
            return z < 0
        end = ((z == 1) & (zi == 0)) | ((z == last - 1) & (zi == last))
        if c >= self.chunks // 2:
            end = end | ((z == 0) & (zi == 1)) | ((z == last) & (zi == last - 1))
        return end

    def copy(self, zi, yi, c, s_sem, r_sem, to_z, to_y):
        ref = self.ref_of(zi * 2 + yi, c)
        return pltpu.make_async_remote_copy(
            src_ref=ref, dst_ref=ref, send_sem=s_sem, recv_sem=r_sem,
            device_id=(to_z * 2 + to_y, self.tp), device_id_type=MESH,
        )

    def up(self, s, c):
        return self.copy(self.z - s, self.y, c, self.up_s.at[s, c], self.up_r.at[s, c], self.z + 1, self.y)

    def down(self, s, c):
        return self.copy(self.z + s, self.y, c, self.dn_s.at[s, c], self.dn_r.at[s, c], self.z - 1, self.y)

    def from_below(self, s, c):
        return self.copy(self.z - 1 - s, self.y, c, self.up_s.at[s, c], self.up_r.at[s, c], self.z, self.y)

    def from_above(self, s, c):
        return self.copy(self.z + 1 + s, self.y, c, self.dn_s.at[s, c], self.dn_r.at[s, c], self.z, self.y)

    def across(self, zi, c):
        return self.copy(zi, self.y, c, self.y_s.at[zi, c], self.y_r.at[zi, c], self.z, 1 - self.y)

    def from_across(self, zi, c):
        return self.copy(zi, 1 - self.y, c, self.y_s.at[zi, c], self.y_r.at[zi, c], self.z, self.y)

    def beside(self, c, to_z):
        return self.copy(self.z, 1 - self.y, c, self.x_s.at[c], self.x_r.at[c], to_z, self.y)

    def from_beside(self, zi, c):
        return self.copy(zi, 1 - self.y, c, self.x_s.at[c], self.x_r.at[c], self.z, self.y)

    def beside_cases(self, c):
        if self.depth < 4:
            return ()
        z, last = self.z, self.depth - 1
        cases = [(z == 0, 1), (z == last, last - 1)]
        if c >= self.chunks // 2:
            cases += [(z == 1, 0), (z == last - 1, last)]
        return cases

    def start(self, c):
        @pl.when(self.goes_up(0))
        def _():
            self.up(0, c).start()

        @pl.when(self.goes_down(0))
        def _():
            self.down(0, c).start()

        if not self.near:
            self.across(self.z, c).start()

    def start_beside(self, c):
        for condition, neighbour in self.beside_cases(c):
            @pl.when(condition)
            def _():
                self.beside(c, neighbour).start()

    def hand_on(self, zi, c):
        @pl.when(jnp.logical_not(self.detour(zi, c)))
        def _():
            self.across(zi, c).start()

    def land(self, zi, c, have):
        gone = self.detour(zi, c)

        @pl.when(gone)
        def _():
            self.from_beside(zi, c).wait_recv()

        @pl.when(jnp.logical_not(gone))
        def _():
            self.from_across(zi, c).wait_recv()

        have(zi * 2 + 1 - self.y, c)

    def relay(self, have=None, after=None):
        have = have or (lambda block, c: None)
        z, depth = self.z, self.depth
        for s in range(1, depth + 1):
            for c in range(self.chunks):
                if s < depth:
                    @pl.when(z - s >= 0)
                    def _():
                        if self.near and s == 1:
                            @pl.when(z != depth - 1)
                            def _():
                                self.from_below(0, c).wait_recv()
                        else:
                            self.from_below(s - 1, c).wait_recv()
                        if s < depth - 1:
                            @pl.when(z + 1 < depth)
                            def _():
                                self.up(s, c).start()
                        self.hand_on(z - s, c)
                        have((z - s) * 2 + self.y, c)

                    @pl.when(z + s < depth)
                    def _():
                        if self.near and s == 1:
                            @pl.when(z != 0)
                            def _():
                                self.from_above(0, c).wait_recv()
                        else:
                            self.from_above(s - 1, c).wait_recv()
                        if s < depth - 1:
                            @pl.when(z >= 1)
                            def _():
                                self.down(s, c).start()
                        self.hand_on(z + s, c)
                        have((z + s) * 2 + self.y, c)

                if s == 1:
                    if not self.near:
                        self.from_across(z, c).wait_recv()
                        self.start_beside(c)
                        have(z * 2 + 1 - self.y, c)
                else:
                    @pl.when(z - (s - 1) >= 0)
                    def _():
                        self.land(z - (s - 1), c, have)

                    @pl.when(z + (s - 1) < depth)
                    def _():
                        self.land(z + (s - 1), c, have)
            if after is not None:
                after(s)

    def finish(self):
        for c in range(self.chunks):
            for s in range(self.depth - 1):
                @pl.when(self.goes_up(s))
                def _():
                    self.up(s, c).wait_send()

                @pl.when(self.goes_down(s))
                def _():
                    self.down(s, c).wait_send()
            for zi in range(self.depth):
                @pl.when(self.crosses(zi, c))
                def _():
                    self.across(zi, c).wait_send()
            for condition, neighbour in self.beside_cases(c):
                @pl.when(condition)
                def _():
                    self.beside(c, neighbour).wait_send()


def gather_sems(depth, chunks):
    dma = pltpu.SemaphoreType.DMA
    return [dma((depth - 1, chunks))] * 4 + [dma((depth, chunks))] * 2 + [dma((chunks,))] * 2


def kernel(
    n, tps, entries,
    saved_hbm, cot_in_hbm, cot_out_hbm, factor_in_hbm, factor_out_hbm, weight_in_hbm, weight_out_hbm,
    first_in_hbm, first_out_hbm, second_in_hbm, second_out_hbm,
    update, fresh, copies, first_new, second_new,
    saved, cots, factors, weights, first, second, mapped, terms, crossed, staged, landed, smalls, squares, early, ahead,
    wy_s, wy_r, wz_s, wz_r, load_sem, pair_s, pair_r, ty_s, ty_r, tz_s, tz_r, sz_s, sz_r, sy_s, sy_r, norm_s, norm_r, *gather_refs,
):
    me, tp = lax.axis_index("fs"), lax.axis_index("tp")
    z, y = me // 2, me % 2
    depth = n // 2
    side = tp % 2
    partner = tp + 1 - 2 * side
    rows = factors.shape[2]
    half = rows // 2
    slim = first.shape[1]
    place = (z, y, tp, depth)

    barrier = pltpu.get_barrier_semaphore()
    for k in range(1, depth):
        pl.semaphore_signal(barrier, inc=1, device_id=((z + k) % depth * 2 + y, tp), device_id_type=MESH)
    pl.semaphore_signal(barrier, inc=1, device_id=(z * 2 + 1 - y, tp), device_id_type=MESH)
    for k in range(1, tps):
        pl.semaphore_signal(barrier, inc=1, device_id=(me, (tp + k) % tps), device_id_type=MESH)

    loads = [
        pltpu.make_async_copy(source, target, load_sem.at[i])
        for i, (source, target) in enumerate((
            (factor_in_hbm, factors.at[0, me]), (factor_out_hbm, factors.at[1, me]),
            (saved_hbm, saved), (cot_in_hbm, cots.at[0]), (cot_out_hbm, cots.at[1]),
            (first_in_hbm, first.at[0]), (first_out_hbm, first.at[1]),
            (second_in_hbm, second.at[0]), (second_out_hbm, second.at[1]),
            (weight_in_hbm, weights.at[0]), (weight_out_hbm, weights.at[1]),
        ))
    ]
    for load in loads:
        load.start()
    loads[0].wait()
    loads[1].wait()
    pl.semaphore_wait(barrier, depth + tps - 1)

    def factor_ref(m, block, c):
        return factors.at[m, block, pl.ds(c * half, half)]

    def hand(m, block, c):
        ref = factor_ref(m, block, c)
        return pltpu.make_async_remote_copy(
            src_ref=ref, dst_ref=ref, send_sem=pair_s.at[block, c], recv_sem=pair_r.at[block, c],
            device_id=(me, partner), device_id_type=MESH,
        )

    gather = Gather(place, 2, lambda block, c: factor_ref(side, block, c), gather_refs[:8])
    gather.start(0)
    gather.start(1)
    loads[2].wait()

    def map_block(block, first_one=False):
        piece = saved[:, pl.ds(pl.multiple_of(block * rows, rows), rows)]
        for m in range(2):
            product = dot(piece, factors[m, block])
            mapped[m] = product if first_one else mapped[m] + product

    def map_handed(block):
        for c in range(2):
            hand(1 - side, block, c).wait_recv()
        map_block(block)

    def map_at(distance):
        if distance == 0:
            map_handed(z * 2 + 1 - y)
            return

        @pl.when(z - distance >= 0)
        def _():
            map_handed((z - distance) * 2 + y)
            map_handed((z - distance) * 2 + 1 - y)

        @pl.when(z + distance < depth)
        def _():
            map_handed((z + distance) * 2 + y)
            map_handed((z + distance) * 2 + 1 - y)

    at_end = (z == 0) | (z == depth - 1)
    inner = jnp.where(z == 0, 1, depth - 2)
    by_end = (z == 1) | (z == depth - 2)
    outer = jnp.where(z == 1, 0, depth - 1)

    def early_cross(m, c):
        return pltpu.make_async_remote_copy(
            src_ref=weights.at[m, pl.ds(c * half, half)], dst_ref=early.at[0, m, pl.ds(c * half, half)],
            send_sem=wy_s.at[m, c], recv_sem=wy_r.at[m, c], device_id=(z * 2 + 1 - y, tp), device_id_type=MESH,
        )

    def early_along(m, c):
        return pltpu.make_async_remote_copy(
            src_ref=weights.at[m, pl.ds(c * half, half)], dst_ref=early.at[1, m, pl.ds(c * half, half)],
            send_sem=wz_s.at[m, c], recv_sem=wz_r.at[m, c], device_id=(outer * 2 + y, tp), device_id_type=MESH,
        )

    def early_along_start(m):
        @pl.when(by_end)
        def _():
            for c in range(2):
                early_along(m, c).start()

    map_block(me, True)
    gather.relay(
        lambda block, c: hand(side, block, c).start(),
        lambda s: map_at(s - 2) if s >= 2 else None,
    )
    for load in loads[3:]:
        load.wait()
    early_cross(0, 0).start()
    early_along_start(0)
    map_at(depth - 1)

    def term_cross(m, zi):
        return pltpu.make_async_remote_copy(
            src_ref=terms.at[m, zi * 2 + 1 - y], dst_ref=crossed.at[m, zi],
            send_sem=ty_s.at[m, zi], recv_sem=ty_r.at[m, zi],
            device_id=(z * 2 + 1 - y, tp), device_id_type=MESH,
        )

    def term_along(m, zi):
        return pltpu.make_async_remote_copy(
            src_ref=staged.at[m, zi], dst_ref=landed.at[m, z], send_sem=tz_s.at[m, zi], recv_sem=tz_r.at[m, z],
            device_id=(zi * 2 + y, tp), device_id_type=MESH,
        )

    def term_from(m, zi):
        return pltpu.make_async_remote_copy(
            src_ref=staged.at[m, z], dst_ref=landed.at[m, zi], send_sem=tz_s.at[m, z], recv_sem=tz_r.at[m, zi],
            device_id=(z * 2 + y, tp), device_id_type=MESH,
        )

    order = [k % depth for k in range(1, depth + 1)]
    for m in range(2):
        high, middle, low = parts_of(mapped[m].T)
        term = dot(high, cots[m]) + (dot(middle, cots[m]) + dot(low, cots[m]))
        terms[m] = term.reshape(n, slim, term.shape[1])
        for k in order:
            term_cross(m, (z + k) % depth).start()
    for m in range(2):
        for k in order:
            zi = (z + k) % depth
            term_cross(m, zi).wait_recv()
            staged[m, zi] = terms[m, zi * 2 + y] + crossed[m, zi]
            if k:
                term_along(m, zi).start()

    early_cross(0, 1).start()

    def small_along(m, zi):
        ref = smalls.at[m, me]
        return pltpu.make_async_remote_copy(
            src_ref=ref, dst_ref=ref, send_sem=sz_s.at[m, zi], recv_sem=sz_r.at[m, z],
            device_id=(zi * 2 + y, tp), device_id_type=MESH,
        )

    def small_from(m, zi):
        ref = smalls.at[m, zi * 2 + y]
        return pltpu.make_async_remote_copy(
            src_ref=ref, dst_ref=ref, send_sem=sz_s.at[m, zi], recv_sem=sz_r.at[m, zi],
            device_id=(z * 2 + y, tp), device_id_type=MESH,
        )

    def small_cross(m, zi, column):
        ref = smalls.at[m, zi * 2 + column]
        return pltpu.make_async_remote_copy(
            src_ref=ref, dst_ref=ref, send_sem=sy_s.at[m, zi], recv_sem=sy_r.at[m, zi],
            device_id=(z * 2 + 1 - y, tp), device_id_type=MESH,
        )

    for m in range(2):
        here = staged[m, z]
        for k in range(1, depth):
            term_from(m, (z + k) % depth).wait_recv()
            here = here + landed[m, (z + k) % depth]
        first_m = 0.8 * first[m] + 0.2 * here
        second_m = 0.9 * second[m] + 0.1 * here * here
        first_new[m] = first_m
        second_new[m] = second_m
        smalls[m, me] = first_m / (jnp.sqrt(second_m) + 1e-08)
        for k in range(1, depth):
            small_along(m, (z + k) % depth).start()
        small_cross(m, z, y).start()
    for m in range(2):
        for k in range(1, depth):
            zi = (z + k) % depth
            small_from(m, zi).wait_recv()
            small_cross(m, zi, y).start()

    def send_square(m, k):
        return pltpu.make_async_remote_copy(
            src_ref=squares.at[m, tp], dst_ref=squares.at[m, tp], send_sem=norm_s.at[m, k], recv_sem=norm_r.at[m, k],
            device_id=(me, (tp + k) % tps), device_id_type=MESH,
        )

    def recv_square(m, k):
        ref = squares.at[m, (tp + tps - k) % tps]
        return pltpu.make_async_remote_copy(
            src_ref=ref, dst_ref=ref, send_sem=norm_s.at[m, k], recv_sem=norm_r.at[m, k],
            device_id=(me, tp), device_id_type=MESH,
        )

    early_cross(1, 0).start()
    early_cross(1, 1).start()
    early_along_start(1)

    def chunk_ref(block, c):
        return copies.at[c // 2, block, pl.ds(c % 2 * half, half)]

    copy_gather = Gather(place, 4, chunk_ref, gather_refs[8:], near=True)
    beside = z * 2 + 1 - y
    behind = inner * 2 + y
    for m in range(2):
        for k in range(depth):
            small_cross(m, (z + k) % depth, 1 - y).wait_recv()
        high, middle, low = parts_of(smalls[m].reshape(n * slim, smalls.shape[3]))

        def full_of(block):
            factor = factors[m, block]
            return dot(factor, high) + (dot(factor, middle) + dot(factor, low))

        total = None
        for block in range(n):
            full = full_of(block)
            square = jnp.sum((full * full).reshape(rows // 8, 8, full.shape[1]), axis=0)
            total = square if total is None else total + square
        squares[m, tp] = total
        for k in range(1, tps):
            send_square(m, k).start()
        update[m] = full_of(me)
        ahead[0] = full_of(beside)

        @pl.when(at_end)
        def _():
            ahead[1] = full_of(behind)

        for k in range(1, tps):
            recv_square(m, k).wait_recv()
        mean = jnp.sum(jnp.sum(squares[m], axis=0), keepdims=True) / entries
        root = jnp.sqrt(mean + 1e-06)
        new_update = update[m] / root
        new_weight = weights[m] - 0.02 * new_update
        copies[m, me] = new_weight.astype(BF16)
        for c in range(2 * m, 2 * m + 2):
            copy_gather.start(c)
        update[m] = new_update
        fresh[m] = new_weight
        for c in range(2):
            early_cross(m, c).wait_recv()
        copies[m, beside] = (early[0, m] - 0.02 * (ahead[0] / root)).astype(BF16)
        for c in range(2 * m, 2 * m + 2):
            copy_gather.start_beside(c)

        @pl.when(at_end)
        def _():
            for c in range(2):
                early_along(m, c).wait_recv()
            copies[m, behind] = (early[1, m] - 0.02 * (ahead[1] / root)).astype(BF16)

    copy_gather.relay()

    for m in range(2):
        for c in range(2):
            early_cross(m, c).wait_send()

            @pl.when(by_end)
            def _():
                early_along(m, c).wait_send()
    gather.finish()
    copy_gather.finish()
    for k in range(1, n):
        for c in range(2):
            hand(side, (me + k) % n, c).wait_send()
    for m in range(2):
        for k in range(depth):
            zi = (z + k) % depth
            term_cross(m, zi).wait_send()
            small_cross(m, zi, y).wait_send()
            if k:
                term_along(m, zi).wait_send()
                small_along(m, zi).wait_send()
        for k in range(1, tps):
            send_square(m, k).wait_send()


def write_kernel(update, fresh, copies, first_new, second_new, *refs):
    outs, sem = refs[:-1], refs[-1]
    started = []
    for i, source in enumerate((update, fresh, copies, first_new, second_new)):
        for m in range(2):
            copy = pltpu.make_async_copy(source.at[m], outs[2 * i + m], sem.at[2 * i + m])
            copy.start()
            started.append(copy)
    for copy in started:
        copy.wait()


def kernel_form(n, tps, saved_input, cot_inproj, cot_outproj, factor_inproj, *others):
    tokens, wide = saved_input.shape
    columns = cot_inproj.shape[1]
    rows, rank = factor_inproj.shape
    slim = rank // n
    depth = n // 2
    entries = float(wide * columns * tps)
    dma = pltpu.SemaphoreType.DMA
    vmem = pl.BlockSpec(memory_space=pltpu.VMEM)
    anywhere = pl.BlockSpec(memory_space=pl.ANY)
    far = pl.BlockSpec(memory_space=pltpu.HBM)
    shape = jax.ShapeDtypeStruct
    results = pl.pallas_call(
        functools.partial(kernel, n, tps, entries),
        out_shape=(
            shape((2, rows, columns), F32), shape((2, rows, columns), F32),
            shape((2, n, rows, columns), BF16),
            shape((2, slim, columns), F32), shape((2, slim, columns), F32),
        ),
        in_specs=[far] * 11,
        out_specs=[vmem] * 5,
        scratch_shapes=[
            pltpu.VMEM((tokens, wide), BF16),
            pltpu.VMEM((2, tokens, columns), BF16),
            pltpu.VMEM((2, n, rows, rank), BF16),
            pltpu.VMEM((2, rows, columns), F32),
            pltpu.VMEM((2, slim, columns), F32),
            pltpu.VMEM((2, slim, columns), F32),
            pltpu.VMEM((2, tokens, rank), F32),
            pltpu.VMEM((2, n, slim, columns), F32),
            pltpu.VMEM((2, depth, slim, columns), F32),
            pltpu.VMEM((2, depth, slim, columns), F32),
            pltpu.VMEM((2, depth, slim, columns), F32),
            pltpu.VMEM((2, n, slim, columns), F32),
            pltpu.VMEM((2, tps, 8, columns), F32),
            pltpu.VMEM((2, 2, rows, columns), F32),
            pltpu.VMEM((2, rows, columns), F32),
            *[dma((2, 2))] * 4,
            dma((11,)),
            dma((n, 2)), dma((n, 2)),
            *[dma((2, depth))] * 8,
            dma((2, tps)), dma((2, tps)),
            *gather_sems(depth, 2), *gather_sems(depth, 4),
        ],
        compiler_params=pltpu.CompilerParams(collective_id=0, has_side_effects=True, vmem_limit_bytes=40 * 2**20),
    )(*[pltpu.with_memory_space_constraint(x, pltpu.HBM) for x in (saved_input, cot_inproj, cot_outproj, factor_inproj, *others)])
    update, fresh, copies, first_new, second_new = results
    copies = copies.reshape(2, n * rows, columns)
    return pl.pallas_call(
        write_kernel,
        out_shape=(
            *[shape((rows, columns), F32)] * 4, *[shape((n * rows, columns), BF16)] * 2, *[shape((slim, columns), F32)] * 4,
        ),
        in_specs=[anywhere] * 5,
        out_specs=[far] * 10,
        scratch_shapes=[dma((10,))],
        compiler_params=pltpu.CompilerParams(vmem_limit_bytes=2**20),
    )(update, fresh, copies, first_new, second_new)


def on_device(saved_input, cot_inproj, cot_outproj, factor_inproj, *others):
    n, tps = lax.axis_size("fs"), lax.axis_size("tp")
    rows, rank = factor_inproj.shape
    if n % 2 == 0 and n >= 8 and tps % 2 == 0 and rank % (8 * n) == 0 and rows % 128 == 0 and cot_inproj.shape[1] % 128 == 0:
        return kernel_form(n, tps, saved_input, cot_inproj, cot_outproj, factor_inproj, *others)
    return plain_form(saved_input, cot_inproj, cot_outproj, factor_inproj, *others)


def solution(mesh):
    return jax.shard_map(
        on_device,
        mesh=mesh,
        in_specs=(
            P("fs", None),
            P("fs", "tp"),
            P("fs", "tp"),
            P("fs", None),
            P("fs", None),
            P("fs", "tp"),
            P("fs", "tp"),
            P("fs", "tp"),
            P("fs", "tp"),
            P("fs", "tp"),
            P("fs", "tp"),
        ),
        out_specs=(
            P("fs", "tp"),
            P("fs", "tp"),
            P("fs", "tp"),
            P("fs", "tp"),
            P(None, "tp"),
            P(None, "tp"),
            P("fs", "tp"),
            P("fs", "tp"),
            P("fs", "tp"),
            P("fs", "tp"),
        ),
        check_vma=False,
    )
```

```python
import functools

import jax
import jax.numpy as jnp
from jax import lax
from jax.experimental import pallas as pl
from jax.experimental.pallas import tpu as pltpu
from jax.sharding import PartitionSpec as P


def contract_rows(left, right, precision):
    return lax.dot_general(
        left,
        right,
        (((0,), (0,)), ((), ())),
        precision=precision,
        preferred_element_type=jnp.float32,
    )


def plain_form(
    saved_input,
    cot_inproj,
    cot_outproj,
    factor_inproj,
    factor_outproj,
    weight_inproj,
    weight_outproj,
    first_inproj,
    first_outproj,
    second_inproj,
    second_outproj,
):
    highest = lax.Precision.HIGHEST
    pieces = (
        lax.all_gather(factor_inproj, "fs", axis=0, tiled=True),
        lax.all_gather(factor_outproj, "fs", axis=0, tiled=True),
    )
    mapped_in = jnp.dot(saved_input, pieces[0], preferred_element_type=jnp.float32)
    mapped_out = jnp.dot(saved_input, pieces[1], preferred_element_type=jnp.float32)
    term_in = contract_rows(mapped_in, cot_inproj.astype(jnp.float32), highest)
    term_out = contract_rows(mapped_out, cot_outproj.astype(jnp.float32), highest)
    projected_in, projected_out = (
        lax.psum_scatter(term_in, "fs", scatter_dimension=0, tiled=True),
        lax.psum_scatter(term_out, "fs", scatter_dimension=0, tiled=True),
    )
    first_in_new = 0.8 * first_inproj + 0.2 * projected_in
    first_out_new = 0.8 * first_outproj + 0.2 * projected_out
    second_in_new = 0.9 * second_inproj + 0.1 * projected_in * projected_in
    second_out_new = 0.9 * second_outproj + 0.1 * projected_out * projected_out
    small_in = first_in_new / (jnp.sqrt(second_in_new) + 1e-08)
    small_out = first_out_new / (jnp.sqrt(second_out_new) + 1e-08)
    wide_in = factor_inproj.astype(jnp.float32)
    wide_out = factor_outproj.astype(jnp.float32)
    pieces = (
        lax.all_gather(small_in, "fs", axis=0, tiled=True),
        lax.all_gather(small_out, "fs", axis=0, tiled=True),
    )
    full_in = jnp.dot(wide_in, pieces[0], precision=highest)
    full_out = jnp.dot(wide_out, pieces[1], precision=highest)
    square_in, square_out = lax.psum(
        (jnp.sum(full_in * full_in), jnp.sum(full_out * full_out)), ("fs", "tp")
    )
    entries = float(full_in.shape[0] * full_in.shape[1] * lax.axis_size("fs") * lax.axis_size("tp"))
    update_in = full_in / jnp.sqrt(square_in / entries + 1e-06)
    update_out = full_out / jnp.sqrt(square_out / entries + 1e-06)
    fresh_in = weight_inproj - 0.02 * update_in
    fresh_out = weight_outproj - 0.02 * update_out
    copy_in, copy_out = (
        lax.all_gather(fresh_in.astype(jnp.bfloat16), "fs", axis=0, tiled=True),
        lax.all_gather(fresh_out.astype(jnp.bfloat16), "fs", axis=0, tiled=True),
    )
    return (
        update_in,
        update_out,
        fresh_in,
        fresh_out,
        copy_in,
        copy_out,
        first_in_new,
        first_out_new,
        second_in_new,
        second_out_new,
    )


MESH = pl.DeviceIdType.MESH
F32, BF16 = jnp.float32, jnp.bfloat16


def parts_of(x):
    high = x.astype(BF16)
    rest = x - high.astype(F32)
    middle = rest.astype(BF16)
    return high, middle, (rest - middle.astype(F32)).astype(BF16)


def dot(a, b):
    return jnp.dot(a, b, preferred_element_type=F32)


class Gather:
    def goes_up(self, s):
        z, last = self.z, self.depth - 1
        needed = (z - s >= 0) & (z < last)
        return needed & (z != last - 1) if self.near and s == 0 else needed

    def goes_down(self, s):
        z, last = self.z, self.depth - 1
        needed = (z + s <= last) & (z >= 1)
        return needed & (z != 1) if self.near and s == 0 else needed

    def crosses(self, zi, c):
        sent = jnp.logical_not(self.detour(zi, c))
        return sent & (zi != self.z) if self.near else sent

    def __init__(self, place, chunks, ref_of, sems, near=False):
        self.z, self.y, self.tp, self.depth = place
        self.near = near
        self.chunks, self.ref_of = chunks, ref_of
        self.up_s, self.up_r, self.dn_s, self.dn_r, self.y_s, self.y_r, self.x_s, self.x_r = sems

    def detour(self, zi, c):
        z, last = self.z, self.depth - 1
        if self.depth < 4:
            return z < 0
        end = ((z == 1) & (zi == 0)) | ((z == last - 1) & (zi == last))
        if c >= self.chunks // 2:
            end = end | ((z == 0) & (zi == 1)) | ((z == last) & (zi == last - 1))
        return end

    def copy(self, zi, yi, c, s_sem, r_sem, to_z, to_y):
        ref = self.ref_of(zi * 2 + yi, c)
        return pltpu.make_async_remote_copy(
            src_ref=ref, dst_ref=ref, send_sem=s_sem, recv_sem=r_sem,
            device_id=(to_z * 2 + to_y, self.tp), device_id_type=MESH,
        )

    def up(self, s, c):
        return self.copy(self.z - s, self.y, c, self.up_s.at[s, c], self.up_r.at[s, c], self.z + 1, self.y)

    def down(self, s, c):
        return self.copy(self.z + s, self.y, c, self.dn_s.at[s, c], self.dn_r.at[s, c], self.z - 1, self.y)

    def from_below(self, s, c):
        return self.copy(self.z - 1 - s, self.y, c, self.up_s.at[s, c], self.up_r.at[s, c], self.z, self.y)

    def from_above(self, s, c):
        return self.copy(self.z + 1 + s, self.y, c, self.dn_s.at[s, c], self.dn_r.at[s, c], self.z, self.y)

    def across(self, zi, c):
        return self.copy(zi, self.y, c, self.y_s.at[zi, c], self.y_r.at[zi, c], self.z, 1 - self.y)

    def from_across(self, zi, c):
        return self.copy(zi, 1 - self.y, c, self.y_s.at[zi, c], self.y_r.at[zi, c], self.z, self.y)

    def beside(self, c, to_z):
        return self.copy(self.z, 1 - self.y, c, self.x_s.at[c], self.x_r.at[c], to_z, self.y)

    def from_beside(self, zi, c):
        return self.copy(zi, 1 - self.y, c, self.x_s.at[c], self.x_r.at[c], self.z, self.y)

    def beside_cases(self, c):
        if self.depth < 4:
            return ()
        z, last = self.z, self.depth - 1
        cases = [(z == 0, 1), (z == last, last - 1)]
        if c >= self.chunks // 2:
            cases += [(z == 1, 0), (z == last - 1, last)]
        return cases

    def start(self, c):
        @pl.when(self.goes_up(0))
        def _():
            self.up(0, c).start()

        @pl.when(self.goes_down(0))
        def _():
            self.down(0, c).start()

        if not self.near:
            self.across(self.z, c).start()

    def start_beside(self, c):
        for condition, neighbour in self.beside_cases(c):
            @pl.when(condition)
            def _():
                self.beside(c, neighbour).start()

    def hand_on(self, zi, c):
        @pl.when(jnp.logical_not(self.detour(zi, c)))
        def _():
            self.across(zi, c).start()

    def land(self, zi, c, have):
        gone = self.detour(zi, c)

        @pl.when(gone)
        def _():
            self.from_beside(zi, c).wait_recv()

        @pl.when(jnp.logical_not(gone))
        def _():
            self.from_across(zi, c).wait_recv()

        have(zi * 2 + 1 - self.y, c)

    def relay(self, have=None, after=None):
        have = have or (lambda block, c: None)
        z, depth = self.z, self.depth
        for s in range(1, depth + 1):
            for c in range(self.chunks):
                if s < depth:
                    @pl.when(z - s >= 0)
                    def _():
                        if self.near and s == 1:
                            @pl.when(z != depth - 1)
                            def _():
                                self.from_below(0, c).wait_recv()
                        else:
                            self.from_below(s - 1, c).wait_recv()
                        if s < depth - 1:
                            @pl.when(z + 1 < depth)
                            def _():
                                self.up(s, c).start()
                        self.hand_on(z - s, c)
                        have((z - s) * 2 + self.y, c)

                    @pl.when(z + s < depth)
                    def _():
                        if self.near and s == 1:
                            @pl.when(z != 0)
                            def _():
                                self.from_above(0, c).wait_recv()
                        else:
                            self.from_above(s - 1, c).wait_recv()
                        if s < depth - 1:
                            @pl.when(z >= 1)
                            def _():
                                self.down(s, c).start()
                        self.hand_on(z + s, c)
                        have((z + s) * 2 + self.y, c)

                if s == 1:
                    if not self.near:
                        self.from_across(z, c).wait_recv()
                        self.start_beside(c)
                        have(z * 2 + 1 - self.y, c)
                else:
                    @pl.when(z - (s - 1) >= 0)
                    def _():
                        self.land(z - (s - 1), c, have)

                    @pl.when(z + (s - 1) < depth)
                    def _():
                        self.land(z + (s - 1), c, have)
            if after is not None:
                after(s)

    def finish(self):
        for c in range(self.chunks):
            for s in range(self.depth - 1):
                @pl.when(self.goes_up(s))
                def _():
                    self.up(s, c).wait_send()

                @pl.when(self.goes_down(s))
                def _():
                    self.down(s, c).wait_send()
            for zi in range(self.depth):
                @pl.when(self.crosses(zi, c))
                def _():
                    self.across(zi, c).wait_send()
            for condition, neighbour in self.beside_cases(c):
                @pl.when(condition)
                def _():
                    self.beside(c, neighbour).wait_send()


def gather_sems(depth, chunks):
    dma = pltpu.SemaphoreType.DMA
    return [dma((depth - 1, chunks))] * 4 + [dma((depth, chunks))] * 2 + [dma((chunks,))] * 2


def kernel(
    n, tps, entries,
    saved_hbm, cot_in_hbm, cot_out_hbm, factor_in_hbm, factor_out_hbm, weight_in_hbm, weight_out_hbm,
    first_in_hbm, first_out_hbm, second_in_hbm, second_out_hbm,
    update, fresh, copies, first_new, second_new,
    saved, cots, factors, weights, first, second, mapped, terms, crossed, staged, landed, smalls, squares, early, ahead,
    wy_s, wy_r, wz_s, wz_r, twin_s, twin_r, load_sem, pair_s, pair_r, ty_s, ty_r, tz_s, tz_r, sz_s, sz_r, sy_s, sy_r, norm_s, norm_r, *gather_refs,
):
    me, tp = lax.axis_index("fs"), lax.axis_index("tp")
    z, y = me // 2, me % 2
    depth = n // 2
    side = tp % 2
    partner = tp + 1 - 2 * side
    rows = factors.shape[2]
    half = rows // 2
    slim = first.shape[1]
    place = (z, y, tp, depth)

    barrier = pltpu.get_barrier_semaphore()
    for k in range(1, depth):
        pl.semaphore_signal(barrier, inc=1, device_id=((z + k) % depth * 2 + y, tp), device_id_type=MESH)
    pl.semaphore_signal(barrier, inc=1, device_id=(z * 2 + 1 - y, tp), device_id_type=MESH)
    for k in range(1, tps):
        pl.semaphore_signal(barrier, inc=1, device_id=(me, (tp + k) % tps), device_id_type=MESH)

    loads = [
        pltpu.make_async_copy(source, target, load_sem.at[i])
        for i, (source, target) in enumerate((
            (factor_in_hbm, factors.at[0, me]), (factor_out_hbm, factors.at[1, me]),
            (saved_hbm, saved), (cot_in_hbm, cots.at[0]), (cot_out_hbm, cots.at[1]),
            (first_in_hbm, first.at[0]), (first_out_hbm, first.at[1]),
            (second_in_hbm, second.at[0]), (second_out_hbm, second.at[1]),
            (weight_in_hbm, weights.at[0]), (weight_out_hbm, weights.at[1]),
        ))
    ]
    for load in loads:
        load.start()
    loads[0].wait()
    loads[1].wait()
    pl.semaphore_wait(barrier, depth + tps - 1)

    quarter = half // 2
    group = tp // 2
    twin = (tp + 2) % tps

    def factor_ref(m, block, h, c):
        return factors.at[m, block, pl.ds(pl.multiple_of(h * half + c * quarter, quarter), quarter)]

    def hand(m, block, h, c):
        ref = factor_ref(m, block, h, c)
        at = h * 2 + c
        return pltpu.make_async_remote_copy(
            src_ref=ref, dst_ref=ref, send_sem=pair_s.at[block, at], recv_sem=pair_r.at[block, at],
            device_id=(me, partner), device_id_type=MESH,
        )

    def share(block, h, c):
        ref = factor_ref(side, block, h, c)
        return pltpu.make_async_remote_copy(
            src_ref=ref, dst_ref=ref, send_sem=twin_s.at[block, c], recv_sem=twin_r.at[block, c],
            device_id=(me, twin), device_id_type=MESH,
        )

    def have_factor(block, c):
        share(block, group, c).start()
        hand(side, block, group, c).start()

    gather = Gather(place, 2, lambda block, c: factor_ref(side, block, group, c), gather_refs[:8])
    gather.start(0)
    gather.start(1)
    loads[2].wait()

    def map_block(block, first_one=False):
        piece = saved[:, pl.ds(pl.multiple_of(block * rows, rows), rows)]
        for m in range(2):
            product = dot(piece, factors[m, block])
            mapped[m] = product if first_one else mapped[m] + product

    def map_handed(*blocks):
        for block in blocks:
            for c in range(2):
                share(block, 1 - group, c).wait_recv()
                hand(side, block, 1 - group, c).start()
        for block in blocks:
            for h in range(2):
                for c in range(2):
                    hand(1 - side, block, h, c).wait_recv()
            map_block(block)

    def map_at(distance):
        if distance == 0:
            map_handed(z * 2 + 1 - y)
            return

        @pl.when(z - distance >= 0)
        def _():
            map_handed((z - distance) * 2 + y, (z - distance) * 2 + 1 - y)

        @pl.when(z + distance < depth)
        def _():
            map_handed((z + distance) * 2 + y, (z + distance) * 2 + 1 - y)

    at_end = (z == 0) | (z == depth - 1)
    inner = jnp.where(z == 0, 1, depth - 2)
    by_end = (z == 1) | (z == depth - 2)
    outer = jnp.where(z == 1, 0, depth - 1)

    def early_cross(m, c):
        return pltpu.make_async_remote_copy(
            src_ref=weights.at[m, pl.ds(c * half, half)], dst_ref=early.at[0, m, pl.ds(c * half, half)],
            send_sem=wy_s.at[m, c], recv_sem=wy_r.at[m, c], device_id=(z * 2 + 1 - y, tp), device_id_type=MESH,
        )

    def early_along(m, c):
        return pltpu.make_async_remote_copy(
            src_ref=weights.at[m, pl.ds(c * half, half)], dst_ref=early.at[1, m, pl.ds(c * half, half)],
            send_sem=wz_s.at[m, c], recv_sem=wz_r.at[m, c], device_id=(outer * 2 + y, tp), device_id_type=MESH,
        )

    def early_along_start(m):
        @pl.when(by_end)
        def _():
            for c in range(2):
                early_along(m, c).start()

    map_block(me, True)
    for load in loads[3:]:
        load.wait()

    def after_step(s):
        if s == depth - 1:
            early_cross(0, 0).start()
            early_cross(0, 1).start()
            early_along_start(0)
        if s >= 2:
            map_at(s - 2)

    gather.relay(have_factor, after_step)
    map_at(depth - 1)

    def term_cross(m, zi):
        return pltpu.make_async_remote_copy(
            src_ref=terms.at[m, zi * 2 + 1 - y], dst_ref=crossed.at[m, zi],
            send_sem=ty_s.at[m, zi], recv_sem=ty_r.at[m, zi],
            device_id=(z * 2 + 1 - y, tp), device_id_type=MESH,
        )

    def term_along(m, zi):
        return pltpu.make_async_remote_copy(
            src_ref=staged.at[m, zi], dst_ref=landed.at[m, z], send_sem=tz_s.at[m, zi], recv_sem=tz_r.at[m, z],
            device_id=(zi * 2 + y, tp), device_id_type=MESH,
        )

    def term_from(m, zi):
        return pltpu.make_async_remote_copy(
            src_ref=staged.at[m, z], dst_ref=landed.at[m, zi], send_sem=tz_s.at[m, z], recv_sem=tz_r.at[m, zi],
            device_id=(z * 2 + y, tp), device_id_type=MESH,
        )

    order = [k % depth for k in range(1, depth + 1)]
    for m in range(2):
        high, middle, low = parts_of(mapped[m].T)
        term = dot(high, cots[m]) + (dot(middle, cots[m]) + dot(low, cots[m]))
        terms[m] = term.reshape(n, slim, term.shape[1])
        for k in order:
            term_cross(m, (z + k) % depth).start()
    for m in range(2):
        for k in order:
            zi = (z + k) % depth
            term_cross(m, zi).wait_recv()
            staged[m, zi] = terms[m, zi * 2 + y] + crossed[m, zi]
            if k:
                term_along(m, zi).start()

    def small_along(m, zi):
        ref = smalls.at[m, me]
        return pltpu.make_async_remote_copy(
            src_ref=ref, dst_ref=ref, send_sem=sz_s.at[m, zi], recv_sem=sz_r.at[m, z],
            device_id=(zi * 2 + y, tp), device_id_type=MESH,
        )

    def small_from(m, zi):
        ref = smalls.at[m, zi * 2 + y]
        return pltpu.make_async_remote_copy(
            src_ref=ref, dst_ref=ref, send_sem=sz_s.at[m, zi], recv_sem=sz_r.at[m, zi],
            device_id=(z * 2 + y, tp), device_id_type=MESH,
        )

    def small_cross(m, zi, column):
        ref = smalls.at[m, zi * 2 + column]
        return pltpu.make_async_remote_copy(
            src_ref=ref, dst_ref=ref, send_sem=sy_s.at[m, zi], recv_sem=sy_r.at[m, zi],
            device_id=(z * 2 + 1 - y, tp), device_id_type=MESH,
        )

    for m in range(2):
        here = staged[m, z]
        for k in range(1, depth):
            term_from(m, (z + k) % depth).wait_recv()
            here = here + landed[m, (z + k) % depth]
        first_m = 0.8 * first[m] + 0.2 * here
        second_m = 0.9 * second[m] + 0.1 * here * here
        first_new[m] = first_m
        second_new[m] = second_m
        smalls[m, me] = first_m / (jnp.sqrt(second_m) + 1e-08)
        for k in range(1, depth):
            small_along(m, (z + k) % depth).start()
        small_cross(m, z, y).start()
    for m in range(2):
        for k in range(1, depth):
            zi = (z + k) % depth
            small_from(m, zi).wait_recv()
            small_cross(m, zi, y).start()

    def send_square(m, k):
        return pltpu.make_async_remote_copy(
            src_ref=squares.at[m, tp], dst_ref=squares.at[m, tp], send_sem=norm_s.at[m, k], recv_sem=norm_r.at[m, k],
            device_id=(me, (tp + k) % tps), device_id_type=MESH,
        )

    def recv_square(m, k):
        ref = squares.at[m, (tp + tps - k) % tps]
        return pltpu.make_async_remote_copy(
            src_ref=ref, dst_ref=ref, send_sem=norm_s.at[m, k], recv_sem=norm_r.at[m, k],
            device_id=(me, tp), device_id_type=MESH,
        )

    early_cross(1, 0).start()
    early_cross(1, 1).start()
    early_along_start(1)

    def chunk_ref(block, c):
        return copies.at[c // 2, block, pl.ds(c % 2 * half, half)]

    copy_gather = Gather(place, 4, chunk_ref, gather_refs[8:], near=True)
    beside = z * 2 + 1 - y
    behind = inner * 2 + y
    for m in range(2):
        for k in range(depth):
            small_cross(m, (z + k) % depth, 1 - y).wait_recv()
        high, middle, low = parts_of(smalls[m].reshape(n * slim, smalls.shape[3]))

        def full_of(block):
            factor = factors[m, block]
            return dot(factor, high) + (dot(factor, middle) + dot(factor, low))

        total = None
        for block in range(n):
            full = full_of(block)
            square = jnp.sum((full * full).reshape(rows // 8, 8, full.shape[1]), axis=0)
            total = square if total is None else total + square
        squares[m, tp] = total
        for k in range(1, tps):
            send_square(m, k).start()
        update[m] = full_of(me)
        ahead[0] = full_of(beside)

        @pl.when(at_end)
        def _():
            ahead[1] = full_of(behind)

        for k in range(1, tps):
            recv_square(m, k).wait_recv()
        mean = jnp.sum(jnp.sum(squares[m], axis=0), keepdims=True) / entries
        root = jnp.sqrt(mean + 1e-06)
        new_update = update[m] / root
        new_weight = weights[m] - 0.02 * new_update
        copies[m, me] = new_weight.astype(BF16)
        for c in range(2 * m, 2 * m + 2):
            copy_gather.start(c)
        update[m] = new_update
        fresh[m] = new_weight
        for c in range(2):
            early_cross(m, c).wait_recv()
        copies[m, beside] = (early[0, m] - 0.02 * (ahead[0] / root)).astype(BF16)
        for c in range(2 * m, 2 * m + 2):
            copy_gather.start_beside(c)

        @pl.when(at_end)
        def _():
            for c in range(2):
                early_along(m, c).wait_recv()
            copies[m, behind] = (early[1, m] - 0.02 * (ahead[1] / root)).astype(BF16)

    copy_gather.relay()

    for m in range(2):
        for c in range(2):
            early_cross(m, c).wait_send()

            @pl.when(by_end)
            def _():
                early_along(m, c).wait_send()
    gather.finish()
    copy_gather.finish()
    for k in range(1, n):
        for c in range(2):
            share((me + k) % n, group, c).wait_send()
            for h in range(2):
                hand(side, (me + k) % n, h, c).wait_send()
    for m in range(2):
        for k in range(depth):
            zi = (z + k) % depth
            term_cross(m, zi).wait_send()
            small_cross(m, zi, y).wait_send()
            if k:
                term_along(m, zi).wait_send()
                small_along(m, zi).wait_send()
        for k in range(1, tps):
            send_square(m, k).wait_send()


def write_kernel(update, fresh, copies, first_new, second_new, *refs):
    outs, sem = refs[:-1], refs[-1]
    started = []
    for i, source in enumerate((update, fresh, copies, first_new, second_new)):
        for m in range(2):
            copy = pltpu.make_async_copy(source.at[m], outs[2 * i + m], sem.at[2 * i + m])
            copy.start()
            started.append(copy)
    for copy in started:
        copy.wait()


def kernel_form(n, tps, saved_input, cot_inproj, cot_outproj, factor_inproj, *others):
    tokens, wide = saved_input.shape
    columns = cot_inproj.shape[1]
    rows, rank = factor_inproj.shape
    slim = rank // n
    depth = n // 2
    entries = float(wide * columns * tps)
    dma = pltpu.SemaphoreType.DMA
    vmem = pl.BlockSpec(memory_space=pltpu.VMEM)
    anywhere = pl.BlockSpec(memory_space=pl.ANY)
    far = pl.BlockSpec(memory_space=pltpu.HBM)
    shape = jax.ShapeDtypeStruct
    results = pl.pallas_call(
        functools.partial(kernel, n, tps, entries),
        out_shape=(
            shape((2, rows, columns), F32), shape((2, rows, columns), F32),
            shape((2, n, rows, columns), BF16),
            shape((2, slim, columns), F32), shape((2, slim, columns), F32),
        ),
        in_specs=[far] * 11,
        out_specs=[vmem] * 5,
        scratch_shapes=[
            pltpu.VMEM((tokens, wide), BF16),
            pltpu.VMEM((2, tokens, columns), BF16),
            pltpu.VMEM((2, n, rows, rank), BF16),
            pltpu.VMEM((2, rows, columns), F32),
            pltpu.VMEM((2, slim, columns), F32),
            pltpu.VMEM((2, slim, columns), F32),
            pltpu.VMEM((2, tokens, rank), F32),
            pltpu.VMEM((2, n, slim, columns), F32),
            pltpu.VMEM((2, depth, slim, columns), F32),
            pltpu.VMEM((2, depth, slim, columns), F32),
            pltpu.VMEM((2, depth, slim, columns), F32),
            pltpu.VMEM((2, n, slim, columns), F32),
            pltpu.VMEM((2, tps, 8, columns), F32),
            pltpu.VMEM((2, 2, rows, columns), F32),
            pltpu.VMEM((2, rows, columns), F32),
            *[dma((2, 2))] * 4,
            dma((n, 2)), dma((n, 2)),
            dma((11,)),
            dma((n, 4)), dma((n, 4)),
            *[dma((2, depth))] * 8,
            dma((2, tps)), dma((2, tps)),
            *gather_sems(depth, 2), *gather_sems(depth, 4),
        ],
        compiler_params=pltpu.CompilerParams(collective_id=0, has_side_effects=True, vmem_limit_bytes=40 * 2**20),
    )(*[pltpu.with_memory_space_constraint(x, pltpu.HBM) for x in (saved_input, cot_inproj, cot_outproj, factor_inproj, *others)])
    update, fresh, copies, first_new, second_new = results
    copies = copies.reshape(2, n * rows, columns)
    return pl.pallas_call(
        write_kernel,
        out_shape=(
            *[shape((rows, columns), F32)] * 4, *[shape((n * rows, columns), BF16)] * 2, *[shape((slim, columns), F32)] * 4,
        ),
        in_specs=[anywhere] * 5,
        out_specs=[far] * 10,
        scratch_shapes=[dma((10,))],
        compiler_params=pltpu.CompilerParams(vmem_limit_bytes=2**20),
    )(update, fresh, copies, first_new, second_new)


def on_device(saved_input, cot_inproj, cot_outproj, factor_inproj, *others):
    n, tps = lax.axis_size("fs"), lax.axis_size("tp")
    rows, rank = factor_inproj.shape
    if n % 2 == 0 and n >= 8 and tps == 4 and rank % (8 * n) == 0 and rows % 128 == 0 and cot_inproj.shape[1] % 128 == 0:
        return kernel_form(n, tps, saved_input, cot_inproj, cot_outproj, factor_inproj, *others)
    return plain_form(saved_input, cot_inproj, cot_outproj, factor_inproj, *others)


def solution(mesh):
    return jax.shard_map(
        on_device,
        mesh=mesh,
        in_specs=(
            P("fs", None),
            P("fs", "tp"),
            P("fs", "tp"),
            P("fs", None),
            P("fs", None),
            P("fs", "tp"),
            P("fs", "tp"),
            P("fs", "tp"),
            P("fs", "tp"),
            P("fs", "tp"),
            P("fs", "tp"),
        ),
        out_specs=(
            P("fs", "tp"),
            P("fs", "tp"),
            P("fs", "tp"),
            P("fs", "tp"),
            P(None, "tp"),
            P(None, "tp"),
            P("fs", "tp"),
            P("fs", "tp"),
            P("fs", "tp"),
            P("fs", "tp"),
        ),
        check_vma=False,
    )
```

```python
import functools

import jax
import jax.numpy as jnp
from jax import lax
from jax.experimental import pallas as pl
from jax.experimental.pallas import tpu as pltpu
from jax.sharding import PartitionSpec as P


def contract_rows(left, right, precision):
    return lax.dot_general(
        left,
        right,
        (((0,), (0,)), ((), ())),
        precision=precision,
        preferred_element_type=jnp.float32,
    )


def plain_form(
    saved_input,
    cot_inproj,
    cot_outproj,
    factor_inproj,
    factor_outproj,
    weight_inproj,
    weight_outproj,
    first_inproj,
    first_outproj,
    second_inproj,
    second_outproj,
):
    highest = lax.Precision.HIGHEST
    pieces = (
        lax.all_gather(factor_inproj, "fs", axis=0, tiled=True),
        lax.all_gather(factor_outproj, "fs", axis=0, tiled=True),
    )
    mapped_in = jnp.dot(saved_input, pieces[0], preferred_element_type=jnp.float32)
    mapped_out = jnp.dot(saved_input, pieces[1], preferred_element_type=jnp.float32)
    term_in = contract_rows(mapped_in, cot_inproj.astype(jnp.float32), highest)
    term_out = contract_rows(mapped_out, cot_outproj.astype(jnp.float32), highest)
    projected_in, projected_out = (
        lax.psum_scatter(term_in, "fs", scatter_dimension=0, tiled=True),
        lax.psum_scatter(term_out, "fs", scatter_dimension=0, tiled=True),
    )
    first_in_new = 0.8 * first_inproj + 0.2 * projected_in
    first_out_new = 0.8 * first_outproj + 0.2 * projected_out
    second_in_new = 0.9 * second_inproj + 0.1 * projected_in * projected_in
    second_out_new = 0.9 * second_outproj + 0.1 * projected_out * projected_out
    small_in = first_in_new / (jnp.sqrt(second_in_new) + 1e-08)
    small_out = first_out_new / (jnp.sqrt(second_out_new) + 1e-08)
    wide_in = factor_inproj.astype(jnp.float32)
    wide_out = factor_outproj.astype(jnp.float32)
    pieces = (
        lax.all_gather(small_in, "fs", axis=0, tiled=True),
        lax.all_gather(small_out, "fs", axis=0, tiled=True),
    )
    full_in = jnp.dot(wide_in, pieces[0], precision=highest)
    full_out = jnp.dot(wide_out, pieces[1], precision=highest)
    square_in, square_out = lax.psum(
        (jnp.sum(full_in * full_in), jnp.sum(full_out * full_out)), ("fs", "tp")
    )
    entries = float(full_in.shape[0] * full_in.shape[1] * lax.axis_size("fs") * lax.axis_size("tp"))
    update_in = full_in / jnp.sqrt(square_in / entries + 1e-06)
    update_out = full_out / jnp.sqrt(square_out / entries + 1e-06)
    fresh_in = weight_inproj - 0.02 * update_in
    fresh_out = weight_outproj - 0.02 * update_out
    copy_in, copy_out = (
        lax.all_gather(fresh_in.astype(jnp.bfloat16), "fs", axis=0, tiled=True),
        lax.all_gather(fresh_out.astype(jnp.bfloat16), "fs", axis=0, tiled=True),
    )
    return (
        update_in,
        update_out,
        fresh_in,
        fresh_out,
        copy_in,
        copy_out,
        first_in_new,
        first_out_new,
        second_in_new,
        second_out_new,
    )


MESH = pl.DeviceIdType.MESH
F32, BF16 = jnp.float32, jnp.bfloat16


def parts_of(x):
    high = x.astype(BF16)
    rest = x - high.astype(F32)
    middle = rest.astype(BF16)
    return high, middle, (rest - middle.astype(F32)).astype(BF16)


def dot(a, b):
    return jnp.dot(a, b, preferred_element_type=F32)


class Gather:
    def goes_up(self, s):
        z, last = self.z, self.depth - 1
        needed = (z - s >= 0) & (z < last)
        return needed & (z != last - 1) if self.near and s == 0 else needed

    def goes_down(self, s):
        z, last = self.z, self.depth - 1
        needed = (z + s <= last) & (z >= 1)
        return needed & (z != 1) if self.near and s == 0 else needed

    def crosses(self, zi, c):
        sent = jnp.logical_not(self.detour(zi, c))
        return sent & (zi != self.z) if self.near else sent

    def __init__(self, place, chunks, ref_of, sems, near=False):
        self.z, self.y, self.tp, self.depth = place
        self.near = near
        self.chunks, self.ref_of = chunks, ref_of
        self.up_s, self.up_r, self.dn_s, self.dn_r, self.y_s, self.y_r, self.x_s, self.x_r = sems

    def detour(self, zi, c):
        z, last = self.z, self.depth - 1
        if self.depth < 4:
            return z < 0
        end = ((z == 1) & (zi == 0)) | ((z == last - 1) & (zi == last))
        if c >= self.chunks // 2:
            end = end | ((z == 0) & (zi == 1)) | ((z == last) & (zi == last - 1))
        return end

    def copy(self, zi, yi, c, s_sem, r_sem, to_z, to_y):
        ref = self.ref_of(zi * 2 + yi, c)
        return pltpu.make_async_remote_copy(
            src_ref=ref, dst_ref=ref, send_sem=s_sem, recv_sem=r_sem,
            device_id=(to_z * 2 + to_y, self.tp), device_id_type=MESH,
        )

    def up(self, s, c):
        return self.copy(self.z - s, self.y, c, self.up_s.at[s, c], self.up_r.at[s, c], self.z + 1, self.y)

    def down(self, s, c):
        return self.copy(self.z + s, self.y, c, self.dn_s.at[s, c], self.dn_r.at[s, c], self.z - 1, self.y)

    def from_below(self, s, c):
        return self.copy(self.z - 1 - s, self.y, c, self.up_s.at[s, c], self.up_r.at[s, c], self.z, self.y)

    def from_above(self, s, c):
        return self.copy(self.z + 1 + s, self.y, c, self.dn_s.at[s, c], self.dn_r.at[s, c], self.z, self.y)

    def across(self, zi, c):
        return self.copy(zi, self.y, c, self.y_s.at[zi, c], self.y_r.at[zi, c], self.z, 1 - self.y)

    def from_across(self, zi, c):
        return self.copy(zi, 1 - self.y, c, self.y_s.at[zi, c], self.y_r.at[zi, c], self.z, self.y)

    def beside(self, c, to_z):
        return self.copy(self.z, 1 - self.y, c, self.x_s.at[c], self.x_r.at[c], to_z, self.y)

    def from_beside(self, zi, c):
        return self.copy(zi, 1 - self.y, c, self.x_s.at[c], self.x_r.at[c], self.z, self.y)

    def beside_cases(self, c):
        if self.depth < 4:
            return ()
        z, last = self.z, self.depth - 1
        cases = [(z == 0, 1), (z == last, last - 1)]
        if c >= self.chunks // 2:
            cases += [(z == 1, 0), (z == last - 1, last)]
        return cases

    def start(self, c):
        @pl.when(self.goes_up(0))
        def _():
            self.up(0, c).start()

        @pl.when(self.goes_down(0))
        def _():
            self.down(0, c).start()

        if not self.near:
            self.across(self.z, c).start()

    def start_beside(self, c):
        for condition, neighbour in self.beside_cases(c):
            @pl.when(condition)
            def _():
                self.beside(c, neighbour).start()

    def hand_on(self, zi, c):
        @pl.when(jnp.logical_not(self.detour(zi, c)))
        def _():
            self.across(zi, c).start()

    def land(self, zi, c, have):
        gone = self.detour(zi, c)

        @pl.when(gone)
        def _():
            self.from_beside(zi, c).wait_recv()

        @pl.when(jnp.logical_not(gone))
        def _():
            self.from_across(zi, c).wait_recv()

        have(zi * 2 + 1 - self.y, c)

    def relay(self, have=None, after=None):
        have = have or (lambda block, c: None)
        z, depth = self.z, self.depth
        for s in range(1, depth + 1):
            for c in range(self.chunks):
                if s < depth:
                    @pl.when(z - s >= 0)
                    def _():
                        if self.near and s == 1:
                            @pl.when(z != depth - 1)
                            def _():
                                self.from_below(0, c).wait_recv()
                        else:
                            self.from_below(s - 1, c).wait_recv()
                        if s < depth - 1:
                            @pl.when(z + 1 < depth)
                            def _():
                                self.up(s, c).start()
                        self.hand_on(z - s, c)
                        have((z - s) * 2 + self.y, c)

                    @pl.when(z + s < depth)
                    def _():
                        if self.near and s == 1:
                            @pl.when(z != 0)
                            def _():
                                self.from_above(0, c).wait_recv()
                        else:
                            self.from_above(s - 1, c).wait_recv()
                        if s < depth - 1:
                            @pl.when(z >= 1)
                            def _():
                                self.down(s, c).start()
                        self.hand_on(z + s, c)
                        have((z + s) * 2 + self.y, c)

                if s == 1:
                    if not self.near:
                        self.from_across(z, c).wait_recv()
                        self.start_beside(c)
                        have(z * 2 + 1 - self.y, c)
                else:
                    @pl.when(z - (s - 1) >= 0)
                    def _():
                        self.land(z - (s - 1), c, have)

                    @pl.when(z + (s - 1) < depth)
                    def _():
                        self.land(z + (s - 1), c, have)
            if after is not None:
                after(s)

    def finish(self):
        for c in range(self.chunks):
            for s in range(self.depth - 1):
                @pl.when(self.goes_up(s))
                def _():
                    self.up(s, c).wait_send()

                @pl.when(self.goes_down(s))
                def _():
                    self.down(s, c).wait_send()
            for zi in range(self.depth):
                @pl.when(self.crosses(zi, c))
                def _():
                    self.across(zi, c).wait_send()
            for condition, neighbour in self.beside_cases(c):
                @pl.when(condition)
                def _():
                    self.beside(c, neighbour).wait_send()


def gather_sems(depth, chunks):
    dma = pltpu.SemaphoreType.DMA
    return [dma((depth - 1, chunks))] * 4 + [dma((depth, chunks))] * 2 + [dma((chunks,))] * 2


def kernel(
    n, tps, entries,
    saved_hbm, cot_in_hbm, cot_out_hbm, factor_in_hbm, factor_out_hbm, weight_in_hbm, weight_out_hbm,
    first_in_hbm, first_out_hbm, second_in_hbm, second_out_hbm,
    update, fresh, copies, first_new, second_new,
    saved, cots, factors, weights, first, second, mapped, terms, crossed, staged, landed, smalls, squares, early, ahead,
    wy_s, wy_r, wz_s, wz_r, load_sem, pair_s, pair_r, ty_s, ty_r, tz_s, tz_r, sz_s, sz_r, sy_s, sy_r, norm_s, norm_r, *gather_refs,
):
    me, tp = lax.axis_index("fs"), lax.axis_index("tp")
    z, y = me // 2, me % 2
    depth = n // 2
    side = tp % 2
    partner = tp + 1 - 2 * side
    rows = factors.shape[2]
    half = rows // 2
    quarter = rows // 4
    slim = first.shape[1]
    place = (z, y, tp, depth)

    barrier = pltpu.get_barrier_semaphore()
    for k in range(1, depth):
        pl.semaphore_signal(barrier, inc=1, device_id=((z + k) % depth * 2 + y, tp), device_id_type=MESH)
    pl.semaphore_signal(barrier, inc=1, device_id=(z * 2 + 1 - y, tp), device_id_type=MESH)
    for k in range(1, tps):
        pl.semaphore_signal(barrier, inc=1, device_id=(me, (tp + k) % tps), device_id_type=MESH)

    loads = [
        pltpu.make_async_copy(source, target, load_sem.at[i])
        for i, (source, target) in enumerate((
            (factor_in_hbm, factors.at[0, me]), (factor_out_hbm, factors.at[1, me]),
            (saved_hbm, saved), (cot_in_hbm, cots.at[0]), (cot_out_hbm, cots.at[1]),
            (first_in_hbm, first.at[0]), (first_out_hbm, first.at[1]),
            (second_in_hbm, second.at[0]), (second_out_hbm, second.at[1]),
            (weight_in_hbm, weights.at[0]), (weight_out_hbm, weights.at[1]),
        ))
    ]
    for load in loads:
        load.start()
    loads[0].wait()
    loads[1].wait()
    pl.semaphore_wait(barrier, depth + tps - 1)

    def factor_ref(m, block, c):
        return factors.at[m, block, pl.ds(c * quarter, quarter)]

    def hand(m, block, c):
        ref = factor_ref(m, block, c)
        return pltpu.make_async_remote_copy(
            src_ref=ref, dst_ref=ref, send_sem=pair_s.at[block, c], recv_sem=pair_r.at[block, c],
            device_id=(me, partner), device_id_type=MESH,
        )

    gather = Gather(place, 4, lambda block, c: factor_ref(side, block, c), gather_refs[:8])
    for c in range(4):
        gather.start(c)
    loads[2].wait()

    def map_block(block, first_one=False):
        piece = saved[:, pl.ds(pl.multiple_of(block * rows, rows), rows)]
        for m in range(2):
            product = dot(piece, factors[m, block])
            mapped[m] = product if first_one else mapped[m] + product

    def map_handed(block):
        for c in range(4):
            hand(1 - side, block, c).wait_recv()
        map_block(block)

    def map_at(distance):
        if distance == 0:
            map_handed(z * 2 + 1 - y)
            return

        @pl.when(z - distance >= 0)
        def _():
            map_handed((z - distance) * 2 + y)
            map_handed((z - distance) * 2 + 1 - y)

        @pl.when(z + distance < depth)
        def _():
            map_handed((z + distance) * 2 + y)
            map_handed((z + distance) * 2 + 1 - y)

    at_end = (z == 0) | (z == depth - 1)
    inner = jnp.where(z == 0, 1, depth - 2)
    by_end = (z == 1) | (z == depth - 2)
    outer = jnp.where(z == 1, 0, depth - 1)

    def early_cross(m, c):
        return pltpu.make_async_remote_copy(
            src_ref=weights.at[m, pl.ds(c * half, half)], dst_ref=early.at[0, m, pl.ds(c * half, half)],
            send_sem=wy_s.at[m, c], recv_sem=wy_r.at[m, c], device_id=(z * 2 + 1 - y, tp), device_id_type=MESH,
        )

    def early_along(m, c):
        return pltpu.make_async_remote_copy(
            src_ref=weights.at[m, pl.ds(c * half, half)], dst_ref=early.at[1, m, pl.ds(c * half, half)],
            send_sem=wz_s.at[m, c], recv_sem=wz_r.at[m, c], device_id=(outer * 2 + y, tp), device_id_type=MESH,
        )

    def early_along_start(m):
        @pl.when(by_end)
        def _():
            for c in range(2):
                early_along(m, c).start()

    map_block(me, True)
    gather.relay(
        lambda block, c: hand(side, block, c).start(),
        lambda s: map_at(s - 2) if s >= 2 else None,
    )
    for load in loads[3:]:
        load.wait()
    early_cross(0, 0).start()
    early_along_start(0)
    map_at(depth - 1)

    def term_cross(m, zi):
        return pltpu.make_async_remote_copy(
            src_ref=terms.at[m, zi * 2 + 1 - y], dst_ref=crossed.at[m, zi],
            send_sem=ty_s.at[m, zi], recv_sem=ty_r.at[m, zi],
            device_id=(z * 2 + 1 - y, tp), device_id_type=MESH,
        )

    def term_along(m, zi):
        return pltpu.make_async_remote_copy(
            src_ref=staged.at[m, zi], dst_ref=landed.at[m, z], send_sem=tz_s.at[m, zi], recv_sem=tz_r.at[m, z],
            device_id=(zi * 2 + y, tp), device_id_type=MESH,
        )

    def term_from(m, zi):
        return pltpu.make_async_remote_copy(
            src_ref=staged.at[m, z], dst_ref=landed.at[m, zi], send_sem=tz_s.at[m, z], recv_sem=tz_r.at[m, zi],
            device_id=(z * 2 + y, tp), device_id_type=MESH,
        )

    order = [k % depth for k in range(1, depth + 1)]
    for m in range(2):
        high, middle, low = parts_of(mapped[m].T)
        term = dot(high, cots[m]) + (dot(middle, cots[m]) + dot(low, cots[m]))
        terms[m] = term.reshape(n, slim, term.shape[1])
        for k in order:
            term_cross(m, (z + k) % depth).start()
    for m in range(2):
        for k in order:
            zi = (z + k) % depth
            term_cross(m, zi).wait_recv()
            staged[m, zi] = terms[m, zi * 2 + y] + crossed[m, zi]
            if k:
                term_along(m, zi).start()

    early_cross(0, 1).start()

    def small_along(m, zi):
        ref = smalls.at[m, me]
        return pltpu.make_async_remote_copy(
            src_ref=ref, dst_ref=ref, send_sem=sz_s.at[m, zi], recv_sem=sz_r.at[m, z],
            device_id=(zi * 2 + y, tp), device_id_type=MESH,
        )

    def small_from(m, zi):
        ref = smalls.at[m, zi * 2 + y]
        return pltpu.make_async_remote_copy(
            src_ref=ref, dst_ref=ref, send_sem=sz_s.at[m, zi], recv_sem=sz_r.at[m, zi],
            device_id=(z * 2 + y, tp), device_id_type=MESH,
        )

    def small_cross(m, zi, column):
        ref = smalls.at[m, zi * 2 + column]
        return pltpu.make_async_remote_copy(
            src_ref=ref, dst_ref=ref, send_sem=sy_s.at[m, zi], recv_sem=sy_r.at[m, zi],
            device_id=(z * 2 + 1 - y, tp), device_id_type=MESH,
        )

    for m in range(2):
        here = staged[m, z]
        for k in range(1, depth):
            term_from(m, (z + k) % depth).wait_recv()
            here = here + landed[m, (z + k) % depth]
        first_m = 0.8 * first[m] + 0.2 * here
        second_m = 0.9 * second[m] + 0.1 * here * here
        first_new[m] = first_m
        second_new[m] = second_m
        smalls[m, me] = first_m / (jnp.sqrt(second_m) + 1e-08)
        for k in range(1, depth):
            small_along(m, (z + k) % depth).start()
        small_cross(m, z, y).start()
    for m in range(2):
        for k in range(1, depth):
            zi = (z + k) % depth
            small_from(m, zi).wait_recv()
            small_cross(m, zi, y).start()

    def send_square(m, k):
        return pltpu.make_async_remote_copy(
            src_ref=squares.at[m, tp], dst_ref=squares.at[m, tp], send_sem=norm_s.at[m, k], recv_sem=norm_r.at[m, k],
            device_id=(me, (tp + k) % tps), device_id_type=MESH,
        )

    def recv_square(m, k):
        ref = squares.at[m, (tp + tps - k) % tps]
        return pltpu.make_async_remote_copy(
            src_ref=ref, dst_ref=ref, send_sem=norm_s.at[m, k], recv_sem=norm_r.at[m, k],
            device_id=(me, tp), device_id_type=MESH,
        )

    early_cross(1, 0).start()
    early_cross(1, 1).start()
    early_along_start(1)

    def chunk_ref(block, c):
        return copies.at[c // 2, block, pl.ds(c % 2 * half, half)]

    copy_gather = Gather(place, 4, chunk_ref, gather_refs[8:], near=True)
    beside = z * 2 + 1 - y
    behind = inner * 2 + y
    for m in range(2):
        for k in range(depth):
            small_cross(m, (z + k) % depth, 1 - y).wait_recv()
        high, middle, low = parts_of(smalls[m].reshape(n * slim, smalls.shape[3]))

        def full_of(block):
            factor = factors[m, block]
            return dot(factor, high) + (dot(factor, middle) + dot(factor, low))

        total = None
        for block in range(n):
            full = full_of(block)
            square = jnp.sum((full * full).reshape(rows // 8, 8, full.shape[1]), axis=0)
            total = square if total is None else total + square
        squares[m, tp] = total
        for k in range(1, tps):
            send_square(m, k).start()
        update[m] = full_of(me)
        ahead[0] = full_of(beside)

        @pl.when(at_end)
        def _():
            ahead[1] = full_of(behind)

        for k in range(1, tps):
            recv_square(m, k).wait_recv()
        mean = jnp.sum(jnp.sum(squares[m], axis=0), keepdims=True) / entries
        root = jnp.sqrt(mean + 1e-06)
        new_update = update[m] / root
        new_weight = weights[m] - 0.02 * new_update
        copies[m, me] = new_weight.astype(BF16)
        for c in range(2 * m, 2 * m + 2):
            copy_gather.start(c)
        update[m] = new_update
        fresh[m] = new_weight
        for c in range(2):
            early_cross(m, c).wait_recv()
        copies[m, beside] = (early[0, m] - 0.02 * (ahead[0] / root)).astype(BF16)
        for c in range(2 * m, 2 * m + 2):
            copy_gather.start_beside(c)

        @pl.when(at_end)
        def _():
            for c in range(2):
                early_along(m, c).wait_recv()
            copies[m, behind] = (early[1, m] - 0.02 * (ahead[1] / root)).astype(BF16)

    copy_gather.relay()

    for m in range(2):
        for c in range(2):
            early_cross(m, c).wait_send()

            @pl.when(by_end)
            def _():
                early_along(m, c).wait_send()
    gather.finish()
    copy_gather.finish()
    for k in range(1, n):
        for c in range(4):
            hand(side, (me + k) % n, c).wait_send()
    for m in range(2):
        for k in range(depth):
            zi = (z + k) % depth
            term_cross(m, zi).wait_send()
            small_cross(m, zi, y).wait_send()
            if k:
                term_along(m, zi).wait_send()
                small_along(m, zi).wait_send()
        for k in range(1, tps):
            send_square(m, k).wait_send()


def write_kernel(update, fresh, copies, first_new, second_new, *refs):
    outs, sem = refs[:-1], refs[-1]
    started = []
    for i, source in enumerate((update, fresh, copies, first_new, second_new)):
        for m in range(2):
            copy = pltpu.make_async_copy(source.at[m], outs[2 * i + m], sem.at[2 * i + m])
            copy.start()
            started.append(copy)
    for copy in started:
        copy.wait()


def kernel_form(n, tps, saved_input, cot_inproj, cot_outproj, factor_inproj, *others):
    tokens, wide = saved_input.shape
    columns = cot_inproj.shape[1]
    rows, rank = factor_inproj.shape
    slim = rank // n
    depth = n // 2
    entries = float(wide * columns * tps)
    dma = pltpu.SemaphoreType.DMA
    vmem = pl.BlockSpec(memory_space=pltpu.VMEM)
    anywhere = pl.BlockSpec(memory_space=pl.ANY)
    far = pl.BlockSpec(memory_space=pltpu.HBM)
    shape = jax.ShapeDtypeStruct
    results = pl.pallas_call(
        functools.partial(kernel, n, tps, entries),
        out_shape=(
            shape((2, rows, columns), F32), shape((2, rows, columns), F32),
            shape((2, n, rows, columns), BF16),
            shape((2, slim, columns), F32), shape((2, slim, columns), F32),
        ),
        in_specs=[far] * 11,
        out_specs=[vmem] * 5,
        scratch_shapes=[
            pltpu.VMEM((tokens, wide), BF16),
            pltpu.VMEM((2, tokens, columns), BF16),
            pltpu.VMEM((2, n, rows, rank), BF16),
            pltpu.VMEM((2, rows, columns), F32),
            pltpu.VMEM((2, slim, columns), F32),
            pltpu.VMEM((2, slim, columns), F32),
            pltpu.VMEM((2, tokens, rank), F32),
            pltpu.VMEM((2, n, slim, columns), F32),
            pltpu.VMEM((2, depth, slim, columns), F32),
            pltpu.VMEM((2, depth, slim, columns), F32),
            pltpu.VMEM((2, depth, slim, columns), F32),
            pltpu.VMEM((2, n, slim, columns), F32),
            pltpu.VMEM((2, tps, 8, columns), F32),
            pltpu.VMEM((2, 2, rows, columns), F32),
            pltpu.VMEM((2, rows, columns), F32),
            *[dma((2, 2))] * 4,
            dma((11,)),
            dma((n, 4)), dma((n, 4)),
            *[dma((2, depth))] * 8,
            dma((2, tps)), dma((2, tps)),
            *gather_sems(depth, 4), *gather_sems(depth, 4),
        ],
        compiler_params=pltpu.CompilerParams(collective_id=0, has_side_effects=True, vmem_limit_bytes=40 * 2**20),
    )(*[pltpu.with_memory_space_constraint(x, pltpu.HBM) for x in (saved_input, cot_inproj, cot_outproj, factor_inproj, *others)])
    update, fresh, copies, first_new, second_new = results
    copies = copies.reshape(2, n * rows, columns)
    return pl.pallas_call(
        write_kernel,
        out_shape=(
            *[shape((rows, columns), F32)] * 4, *[shape((n * rows, columns), BF16)] * 2, *[shape((slim, columns), F32)] * 4,
        ),
        in_specs=[anywhere] * 5,
        out_specs=[far] * 10,
        scratch_shapes=[dma((10,))],
        compiler_params=pltpu.CompilerParams(vmem_limit_bytes=2**20),
    )(update, fresh, copies, first_new, second_new)


def on_device(saved_input, cot_inproj, cot_outproj, factor_inproj, *others):
    n, tps = lax.axis_size("fs"), lax.axis_size("tp")
    rows, rank = factor_inproj.shape
    if n % 2 == 0 and n >= 8 and tps % 2 == 0 and rank % (8 * n) == 0 and rows % 128 == 0 and cot_inproj.shape[1] % 128 == 0:
        return kernel_form(n, tps, saved_input, cot_inproj, cot_outproj, factor_inproj, *others)
    return plain_form(saved_input, cot_inproj, cot_outproj, factor_inproj, *others)


def solution(mesh):
    return jax.shard_map(
        on_device,
        mesh=mesh,
        in_specs=(
            P("fs", None),
            P("fs", "tp"),
            P("fs", "tp"),
            P("fs", None),
            P("fs", None),
            P("fs", "tp"),
            P("fs", "tp"),
            P("fs", "tp"),
            P("fs", "tp"),
            P("fs", "tp"),
            P("fs", "tp"),
        ),
        out_specs=(
            P("fs", "tp"),
            P("fs", "tp"),
            P("fs", "tp"),
            P("fs", "tp"),
            P(None, "tp"),
            P(None, "tp"),
            P("fs", "tp"),
            P("fs", "tp"),
            P("fs", "tp"),
            P("fs", "tp"),
        ),
        check_vma=False,
    )
```
